768 devices in a mesh: ep: 48 (over z, x), tp: 16 (over y, core).
Axes of the slice: x: 4, y: 8, z: 12, core: 2. Of those that a mesh axis runs over, the one named last changes fastest.
Arguments:
- tokens: bfloat16 [768, 2048], P('ep'), may hold values from -6 to 6
- attn_gain: bfloat16 [2048], replicated, may hold values from 0.099609375 to 1.8984375
- ffn_gain: bfloat16 [2048], replicated, may hold values from 0.099609375 to 1.8984375
- w_query: bfloat16 [2048, 2048], P(None, 'tp'), may hold values from -0.125 to 0.125
- w_key: bfloat16 [2048, 256], replicated, may hold values from -0.125 to 0.125
- w_value: bfloat16 [2048, 256], replicated, may hold values from -0.125 to 0.125
- w_forget: bfloat16 [2048, 32], replicated, may hold values from -0.125 to 0.125
- forget_bias: float32 [32], replicated, may hold values from -1 to 3
- w_out: bfloat16 [2048, 2048], P(None, 'tp'), may hold values from -0.375 to 0.375
- cache_keys: bfloat16 [768, 2048, 256], P(('ep', 'tp')), may hold values from -800 to 800
- cache_values: bfloat16 [768, 2048, 256], P(('ep', 'tp')), may hold values from -6 to 6
- cache_logcum: float32 [768, 32, 2048], P(('ep', 'tp')), as said below
- cache_len: int32 [768], P(('ep', 'tp')), may hold values from 256 to 2048
- route_group: int32 [768], P('ep'), may hold values from 0 to 3, as said below
- route_expert: int32 [768, 2], P('ep'), may hold values from 0 to 11, as said below
- route_weight: float32 [768, 2], P('ep'), may hold values from 0.2 to 1
- w_gate: bfloat16 [48, 2048, 2048], P('ep', None, 'tp'), may hold values from -0.125 to 0.125
- w_up: bfloat16 [48, 2048, 2048], P('ep', None, 'tp'), may hold values from -0.125 to 0.125
- w_down: bfloat16 [48, 2048, 2048], P('ep', None, 'tp'), may hold values from -0.125 to 0.125
Outputs:
- layer_out: bfloat16 [768, 2048], P('ep', 'tp')
The draws below stay inside these ranges and needn't reach their ends.
Inputs may be any that keep to these rules, and one draw needn't show every extreme that they name: Expert groups. Among the 16 sequences of one index of ep no expert route_group * 12 + route_expert is named more than 2 times, and in every draw one expert is named exactly 2 times by the sequences of every index of ep. `route_expert`: the 2 numbers of a sequence differ. `cache_logcum`: each entry is the sum of the log forget gates of that head from the first cached position up to and including that position.
All inputs are finite; a program needn't handle non-finite values.
Results may differ from the reference program's by a relative error of at most 0.012.
The reference program's roundings to bfloat16 on the way count: a program that leaves them out, or rounds other values in their place, can miss the bound.
Values may be sent and summed in bfloat16 or wider, within the bound.
No kernel may reach another device: no remote copies, remote signals or barrier semaphores. Data moves between devices by JAX's collectives and lax.ppermute only.
A program may use at most 32 MiB of HBM per device.

```python
import math
import jax
import jax.numpy as jnp
from jax import lax

D = 2048
QUERY_HEAD_COUNT = 32
KV_HEADS = 4
HEAD = 64
FE = 2048
GROUPS = 4
TOP = 2
CACHE_LENGTH = 2048
GROUP_SEQS = 16
SEQUENCE_TOTAL = 768
EXPERTS = 48
CAP = 2
N_EP = 48


def draw_cache_keys(key, part):
    random_subkeys = jax.random.split(jax.random.fold_in(key, 3), 1)
    base_keys = jnp.clip(jax.random.normal(random_subkeys[0], (SEQUENCE_TOTAL, CACHE_LENGTH, KV_HEADS * HEAD), jnp.float32), -6.0, 6.0)
    return base_keys.astype(jnp.bfloat16)


def draw_cache_logcum(key, part):
    random_subkeys = jax.random.split(jax.random.fold_in(key, 5), 8)
    slow_heads = jax.random.bernoulli(random_subkeys[0], 0.5, (QUERY_HEAD_COUNT,))
    jitter = jnp.exp(jax.random.uniform(random_subkeys[6], (SEQUENCE_TOTAL, QUERY_HEAD_COUNT, CACHE_LENGTH), jnp.float32, math.log(0.3), math.log(3.0)))
    slow_rate = jnp.exp(jax.random.uniform(random_subkeys[1], (QUERY_HEAD_COUNT,), jnp.float32, math.log(0.2), math.log(0.6))) / CACHE_LENGTH
    fast_rate = 1.0 / jnp.exp(jax.random.uniform(random_subkeys[2], (QUERY_HEAD_COUNT,), jnp.float32, math.log(30.0), math.log(100.0)))
    decay_rate = jnp.where(slow_heads, slow_rate, fast_rate)
    seq_factor = jnp.exp(jax.random.uniform(random_subkeys[3], (SEQUENCE_TOTAL, 1, 1), jnp.float32, math.log(0.5), math.log(2.0)))
    block_factor = jnp.exp(jax.random.uniform(random_subkeys[4], (SEQUENCE_TOTAL, 1, 16), jnp.float32, math.log(0.7), math.log(1.4)))
    cache_position = jnp.arange(CACHE_LENGTH)
    block_index = cache_position * 16 // CACHE_LENGTH
    block_scale = block_factor[:, :, block_index]
    step_increments = -decay_rate[None, :, None] * seq_factor * block_scale * jitter
    spike_events = jax.random.randint(random_subkeys[5], (SEQUENCE_TOTAL, 3), 0, CACHE_LENGTH)
    spike_penalty = jnp.log(jax.random.uniform(random_subkeys[7], (SEQUENCE_TOTAL, 3), jnp.float32, 0.5, 0.8))
    match_counts = (cache_position[None, None, :] == spike_events[:, :, None]).astype(jnp.float32)
    step_increments = step_increments + jnp.sum(match_counts * spike_penalty[:, :, None], axis=1)[:, None, :]
    return jnp.cumsum(step_increments, axis=-1)


def routing_draw(key):
    random_subkeys = jax.random.split(key, 6)
    per_group = EXPERTS // GROUPS
    heavy_group = jax.random.randint(random_subkeys[0], (), 0, GROUPS)
    heavy_perm = jax.random.permutation(random_subkeys[1], per_group)
    fewest_rows = per_group * (CAP - 1) // TOP + 1
    heavy_rows = min(per_group * CAP // TOP, GROUP_SEQS)
    heavy_count = jax.random.randint(random_subkeys[2], (N_EP, 1), fewest_rows, heavy_rows + 1)
    row_order = jax.vmap(lambda subkey: jax.random.permutation(subkey, GROUP_SEQS))(jax.random.split(random_subkeys[3], N_EP))
    other_group = (heavy_group + 1 + jax.random.randint(random_subkeys[4], (N_EP, GROUP_SEQS), 0, GROUPS - 1)) % GROUPS
    group_ids = jnp.where(row_order < heavy_count, heavy_group, other_group)
    same_group = group_ids[:, :, None] == group_ids[:, None, :]
    earlier = row_order[:, None, :] < row_order[:, :, None]
    rank_in_group = jnp.sum((same_group & earlier).astype(jnp.int32), axis=2)
    group_perms = jax.vmap(lambda subkey: jax.random.permutation(subkey, per_group))(jax.random.split(random_subkeys[5], N_EP * GROUPS))
    group_perms = group_perms.reshape(N_EP, GROUPS, per_group)
    group_perms = jnp.where(jnp.arange(GROUPS)[None, :, None] == heavy_group, heavy_perm[None, None, :], group_perms)
    row_table = jnp.take_along_axis(group_perms, group_ids[:, :, None], axis=1)
    picks = []
    for choice_index in range(TOP):
        slot_index = (TOP * rank_in_group + choice_index) % per_group
        picks.append(jnp.take_along_axis(row_table, slot_index[:, :, None], axis=2)[:, :, 0])
    experts_local = jnp.stack(picks, axis=-1)
    return (group_ids.reshape(SEQUENCE_TOTAL).astype(jnp.int32), experts_local.reshape(SEQUENCE_TOTAL, TOP).astype(jnp.int32))


def draw_route_group(key, part):
    return routing_draw(jax.random.fold_in(key, 17))[0]


def draw_route_expert(key, part):
    return routing_draw(jax.random.fold_in(key, 17))[1]


def place_ends(values, key, low, largest):
    longest = values.shape.index(max(values.shape))
    spots = []
    for shift in (0, 1):
        where = [jax.random.randint(jax.random.fold_in(key, axis), (), 0, length) for axis, length in enumerate(values.shape)]
        where[longest] = (where[longest] + shift) % values.shape[longest]
        spots.append(tuple(where))
    return values.at[spots[0]].set(low).at[spots[1]].set(largest)


def level_of(rng, extent, cuts, least, largest):
    factor_of = 1.0
    for dim, blocks in cuts:
        steps = jax.random.uniform(jax.random.fold_in(jax.random.fold_in(rng, 6), dim), (blocks,), jnp.float32, least / len(cuts), largest / len(cuts))
        factor_of = factor_of * jnp.repeat(jnp.exp(steps), extent[dim] // blocks).reshape((-1,) + (1,) * (len(extent) - 1 - dim))
    return factor_of


def centred(key, shape, scale, limit, cuts=(), kind=jnp.bfloat16):
    drawn = scale * jax.random.normal(key, shape, jnp.float32)
    if cuts:
        drawn = drawn * level_of(key, shape, cuts, -0.22, 0.18)
    return jnp.clip(drawn, -limit, limit).astype(kind)


def setup_inputs(seed: int = 0) -> dict:
    streams_of = jax.random.split(jax.random.key(seed), 20)
    tokens = centred(streams_of[0], (SEQUENCE_TOTAL, D), 1.0, 6.0, ((0, 48),))
    attn_gain = jnp.clip(1.0 + 0.18 * jax.random.normal(streams_of[1], (D,), jnp.float32), 0.099609375, 1.8984375).astype(jnp.bfloat16)
    ffn_gain = jnp.clip(1.0 + 0.18 * jax.random.normal(streams_of[2], (D,), jnp.float32), 0.099609375, 1.8984375).astype(jnp.bfloat16)
    w_query = centred(streams_of[3], (D, QUERY_HEAD_COUNT * HEAD), D ** -0.5, 0.125, ((1, 16),))
    w_key = centred(streams_of[4], (D, KV_HEADS * HEAD), D ** -0.5, 0.125)
    w_value = centred(streams_of[5], (D, KV_HEADS * HEAD), D ** -0.5, 0.125)
    w_forget = centred(streams_of[6], (D, QUERY_HEAD_COUNT), D ** -0.5, 0.125)
    forget_bias = jnp.clip(jax.random.uniform(streams_of[7], (QUERY_HEAD_COUNT,), jnp.float32, -1.0, 3.0), -1.0, 3.0)
    w_out = centred(streams_of[8], (QUERY_HEAD_COUNT * HEAD, D), (QUERY_HEAD_COUNT * HEAD // 8) ** -0.5, 0.375, ((1, 16),))
    cache_keys = draw_cache_keys(jax.random.fold_in(streams_of[19], 71), 0)
    cache_values = centred(streams_of[10], (SEQUENCE_TOTAL, CACHE_LENGTH, KV_HEADS * HEAD), 1.0, 6.0, ((0, 768),))
    cache_logcum = draw_cache_logcum(jax.random.fold_in(streams_of[19], 71), 0)
    cache_len = place_ends(jax.random.randint(streams_of[12], (SEQUENCE_TOTAL,), CACHE_LENGTH // 8, CACHE_LENGTH + 1), jax.random.fold_in(streams_of[12], 1), CACHE_LENGTH // 8, CACHE_LENGTH).astype(jnp.int32)
    route_group = draw_route_group(jax.random.fold_in(streams_of[19], 71), 0)
    route_expert = draw_route_expert(jax.random.fold_in(streams_of[19], 71), 0)
    route_weight = jnp.clip(jnp.exp(math.log(1.0) - 1.609438 * jax.random.uniform(streams_of[15], (SEQUENCE_TOTAL, TOP), jnp.float32) ** level_of(streams_of[15], (SEQUENCE_TOTAL, TOP), ((0, 48),), -0.2, 0.2)), 0.2, 1.0)
    w_gate = centred(streams_of[16], (EXPERTS, D, FE), D ** -0.5, 0.125, ((0, 48), (2, 16)))
    w_up = centred(streams_of[17], (EXPERTS, D, FE), D ** -0.5, 0.125, ((0, 48), (2, 16)))
    w_down = centred(streams_of[18], (EXPERTS, FE, D), FE ** -0.5, 0.125, ((0, 48), (2, 16)))
    return dict(tokens=tokens, attn_gain=attn_gain, ffn_gain=ffn_gain, w_query=w_query, w_key=w_key, w_value=w_value, w_forget=w_forget, forget_bias=forget_bias, w_out=w_out, cache_keys=cache_keys, cache_values=cache_values, cache_logcum=cache_logcum, cache_len=cache_len, route_group=route_group, route_expert=route_expert, route_weight=route_weight, w_gate=w_gate, w_up=w_up, w_down=w_down)


NORM_EPSILON = 1e-06
MASKED_SCORE = -1e+30

def normalize(values, gain_vec):
    return values * lax.rsqrt(lax.optimization_barrier(jnp.mean(values * values, axis=-1, keepdims=True)) + NORM_EPSILON) * gain_vec.astype(jnp.float32)

def attend_block(arguments):
    query, key_new, value_new, log_gate, keys, cached_values, logcum, lengths = arguments
    count_of_rows = query.shape[0]
    length = keys.shape[1]
    per_kv = QUERY_HEAD_COUNT // KV_HEADS
    score_scale = HEAD ** (-0.5)
    query_float = query.astype(jnp.float32).reshape(count_of_rows, KV_HEADS, per_kv, HEAD)
    keys_f = keys.astype(jnp.float32).reshape(count_of_rows, length, KV_HEADS, HEAD)
    scores = jnp.einsum('bkgd,blkd->bkgl', query_float, keys_f).reshape(count_of_rows, QUERY_HEAD_COUNT, length) * score_scale
    latest = jnp.take_along_axis(logcum, (lengths - 1).astype(jnp.int32)[:, None, None], axis=2)
    scores = scores + latest + log_gate[:, :, None] - logcum
    usable = jnp.arange(length, dtype=jnp.int32)[None, None, :] < lengths[:, None, None]
    scores = jnp.where(usable, scores, MASKED_SCORE)
    current_key = key_new.astype(jnp.float32).reshape(count_of_rows, KV_HEADS, HEAD)
    current_score = jnp.einsum('cnpx,cnx->cnp', query_float, current_key).reshape(count_of_rows, QUERY_HEAD_COUNT) * score_scale
    peak = jnp.maximum(lax.optimization_barrier(jnp.max(scores, axis=2)), current_score)
    weights = jnp.where(usable, jnp.exp(scores - peak[:, :, None]), 0.0)
    own_weight = jnp.exp(current_score - peak)
    denominator = lax.optimization_barrier(jnp.sum(weights, axis=2)) + own_weight
    weights_b = lax.optimization_barrier(weights.astype(jnp.bfloat16)).astype(jnp.float32)
    own_b = lax.optimization_barrier(own_weight.astype(jnp.bfloat16)).astype(jnp.float32)
    values_f = cached_values.astype(jnp.float32).reshape(count_of_rows, length, KV_HEADS, HEAD)
    summed = jnp.einsum('bkgl,blkd->bkgd', weights_b.reshape(count_of_rows, KV_HEADS, per_kv, length), values_f)
    own_value = value_new.astype(jnp.float32).reshape(count_of_rows, KV_HEADS, 1, HEAD)
    summed = summed + own_b.reshape(count_of_rows, KV_HEADS, per_kv)[..., None] * own_value
    summed = summed.reshape(count_of_rows, QUERY_HEAD_COUNT, HEAD) / denominator[:, :, None]
    return summed.reshape(count_of_rows, QUERY_HEAD_COUNT * HEAD).astype(jnp.bfloat16)

def reference(tokens, attn_gain, ffn_gain, w_query, w_key, w_value, w_forget, forget_bias, w_out, cache_keys, cache_values, cache_logcum, cache_len, route_group, route_expert, route_weight, w_gate, w_up, w_down):
    stream = tokens.astype(jnp.float32)
    normed = normalize(stream, attn_gain).astype(jnp.bfloat16)
    query = jnp.dot(normed, w_query, preferred_element_type=jnp.float32).astype(jnp.bfloat16)
    key_new = jnp.dot(normed, w_key, preferred_element_type=jnp.float32).astype(jnp.bfloat16)
    value_new = jnp.dot(normed, w_value, preferred_element_type=jnp.float32).astype(jnp.bfloat16)
    log_gate = jax.nn.log_sigmoid(jnp.dot(normed, w_forget, preferred_element_type=jnp.float32) + forget_bias.astype(jnp.float32))

    def by_group(array):
        return array.reshape((N_EP, GROUP_SEQS) + array.shape[1:])
    pieces = tuple((by_group(array) for array in (query, key_new, value_new, log_gate, cache_keys, cache_values, cache_logcum, cache_len)))
    attended = lax.map(attend_block, pieces).reshape(SEQUENCE_TOTAL, QUERY_HEAD_COUNT * HEAD)
    mixed = (stream + jnp.dot(attended, w_out, preferred_element_type=jnp.float32)).astype(jnp.bfloat16)
    inputs = normalize(mixed.astype(jnp.float32), ffn_gain).astype(jnp.bfloat16)
    experts_per_group = EXPERTS // GROUPS
    picked_ids = (route_group[:, None] * experts_per_group + route_expert).reshape(-1).astype(jnp.int32)
    max_rows = N_EP * CAP
    pick_count = SEQUENCE_TOTAL * TOP

    def one_expert(collected, expert_item):
        gate_weight, up_weight, down_weight, expert_index = expert_item
        chosen = jnp.nonzero(picked_ids == expert_index, size=max_rows, fill_value=pick_count)[0]
        row_data = inputs[jnp.minimum(chosen, pick_count - 1) // TOP]
        gate_proj = jnp.dot(row_data, gate_weight, preferred_element_type=jnp.float32)
        up_proj = jnp.dot(row_data, up_weight, preferred_element_type=jnp.float32)
        hidden = (jax.nn.silu(gate_proj) * up_proj).astype(jnp.bfloat16)
        result = jnp.dot(hidden, down_weight, preferred_element_type=jnp.float32).astype(jnp.bfloat16)
        result = lax.optimization_barrier(result).astype(jnp.float32)
        return (collected.at[chosen].set(result, mode='drop'), None)
    expert_order = jnp.arange(EXPERTS, dtype=jnp.int32)
    picked, _ = lax.scan(one_expert, jnp.zeros((pick_count, D), jnp.float32), (w_gate, w_up, w_down, expert_order))
    moe_sum = lax.optimization_barrier(jnp.sum(route_weight.astype(jnp.float32)[:, :, None] * picked.reshape(SEQUENCE_TOTAL, TOP, D), axis=1))
    return (mixed.astype(jnp.float32) + moe_sum).astype(jnp.bfloat16)
```

```python
import jax
import jax.numpy as jnp
from jax import lax
from jax.experimental import pallas as pl
from jax.experimental.pallas import tpu as pltpu
from jax.sharding import Mesh
from jax.sharding import PartitionSpec as P

QUERY_HEAD_COUNT = 32
KV_HEADS = 4
HEAD = 64
GROUPS = 4
TOP = 2
NORM_EPSILON = 1e-06
MASKED_SCORE = -1e30
CORES = 2
VMEM_LIMIT = 8 * 1024 * 1024

F32 = jnp.float32
BF16 = jnp.bfloat16
VM = pl.BlockSpec(memory_space=pltpu.VMEM)
SM = pl.BlockSpec(memory_space=pltpu.SMEM)


def call(body, outs, operands, specs, scratch=(), flops=1_000_000, moved=1_000_000):
    return pl.pallas_call(
        body,
        out_shape=outs,
        in_specs=specs,
        out_specs=jax.tree.map(lambda _: VM, outs),
        scratch_shapes=list(scratch),
        compiler_params=pltpu.CompilerParams(vmem_limit_bytes=VMEM_LIMIT),
        cost_estimate=pl.CostEstimate(flops=flops, bytes_accessed=moved, transcendentals=0),
    )(*operands)


def shaped(shape, dtype):
    return jax.ShapeDtypeStruct(shape, dtype)


def query_kernel(tokens_ref, gain_ref, w_ref, normed_ref, query_ref):
    values = tokens_ref[...].astype(F32)
    mean = jnp.mean(values * values, axis=-1, keepdims=True)
    scaled = values * lax.rsqrt(mean + NORM_EPSILON)
    lanes = gain_ref.shape[1]
    normed = jnp.concatenate(
        [
            (scaled[:, i * lanes : (i + 1) * lanes] * gain_ref[i : i + 1].astype(F32)).astype(BF16)
            for i in range(gain_ref.shape[0])
        ],
        axis=1,
    )
    normed_ref[...] = normed
    query_ref[...] = jnp.dot(normed, w_ref[...], preferred_element_type=F32).astype(BF16)


def side_kernel(
    place_ref,
    normed_ref,
    w_key_ref,
    w_value_ref,
    w_forget_ref,
    bias_ref,
    group_ref,
    expert_ref,
    weight_ref,
    key_ref,
    value_ref,
    gate_ref,
    send_ref,
    combine_ref,
    *,
    per_group,
):
    place = place_ref[0]
    normed = normed_ref[...]
    rows = normed.shape[0]
    own_row = lax.broadcasted_iota(jnp.int32, (rows, 1), 0) == place

    def projected(w_ref):
        full = jnp.dot(normed, w_ref[...], preferred_element_type=F32)
        return jnp.sum(jnp.where(own_row, full, 0.0), axis=0, keepdims=True)

    key_ref[...] = projected(w_key_ref).astype(BF16).astype(F32)
    value_ref[...] = projected(w_value_ref).astype(BF16).astype(F32)
    logits = lax.dot_general(
        w_forget_ref[...], normed, (((1,), (1,)), ((), ())), preferred_element_type=F32
    )
    heads = logits.shape[0]
    own_column = lax.broadcasted_iota(jnp.int32, (1, rows), 1) == place
    logit = jnp.sum(jnp.where(own_column, logits, 0.0), axis=1, keepdims=True)
    diagonal = lax.broadcasted_iota(jnp.int32, (heads, heads), 0) == lax.broadcasted_iota(
        jnp.int32, (heads, heads), 1
    )
    bias = jnp.sum(jnp.where(diagonal, bias_ref[...], 0.0), axis=1, keepdims=True)
    logit = logit + bias
    log_gate = jnp.minimum(logit, 0.0) - jnp.log1p(jnp.exp(-jnp.abs(logit)))
    gate_ref[...] = jnp.broadcast_to(log_gate, gate_ref.shape)

    picked = group_ref[...] * per_group + expert_ref[...]
    row_index = lax.broadcasted_iota(jnp.int32, (rows, rows), 0)
    column_index = lax.broadcasted_iota(jnp.int32, (rows, rows), 1)
    lines = [picked[j : j + 1] for j in range(TOP)]
    columns = [
        jnp.sum(jnp.where(row_index == column_index, line, 0), axis=1, keepdims=True)
        for line in lines
    ]
    slots, _ = send_ref.shape
    slot_index = lax.broadcasted_iota(jnp.int32, (slots, rows), 0)
    send = jnp.zeros((slots, rows), F32)
    combine = jnp.zeros((slots, rows), F32)
    for j in range(TOP):
        earlier = jnp.zeros((1, rows), jnp.int32)
        for other in columns:
            same = (other == lines[j]) & (row_index < column_index)
            earlier = earlier + jnp.sum(same.astype(jnp.int32), axis=0, keepdims=True)
        hit = slot_index == lines[j] * TOP + earlier
        send = send + jnp.where(hit, 1.0, 0.0)
        combine = combine + jnp.where(hit, weight_ref[j : j + 1], 0.0)
    send_ref[...] = send.astype(BF16)
    combine_ref[...] = combine


def attend_kernel(
    length_ref, query_ref, key_new_ref, value_new_ref, gate_ref, keys_ref, values_ref, cum_ref, out_ref
):
    heads = QUERY_HEAD_COUNT
    pairs = heads // 2
    width = KV_HEADS * HEAD
    used = length_ref[0]

    def index(shape, dim):
        return lax.broadcasted_iota(jnp.int32, shape, dim)

    to_heads = (index((heads, pairs), 0) // 2 == index((heads, pairs), 1)).astype(BF16)
    to_pairs = (index((pairs, heads), 1) // 2 == index((pairs, heads), 0)).astype(BF16)
    doubled = jnp.dot(to_heads, query_ref[...], preferred_element_type=F32)
    odd_row = index((heads, HEAD), 0) % 2 == 1
    one_head = jnp.where(odd_row, doubled[:, HEAD:], doubled[:, :HEAD])
    in_block = index((heads, width), 1) // HEAD == index((heads, width), 0) // (heads // KV_HEADS)
    query_wide = jnp.where(in_block, jnp.concatenate([one_head] * KV_HEADS, axis=1), 0.0)
    query_all = query_wide.astype(BF16)
    scores = lax.dot_general(
        query_all, keys_ref[0], (((1,), (1,)), ((), ())), preferred_element_type=F32
    )
    cum = cum_ref[0]
    log_gate = gate_ref[:, :1]
    position = lax.broadcasted_iota(jnp.int32, scores.shape, 1)
    latest = jnp.sum(jnp.where(position == used - 1, cum, 0.0), axis=1, keepdims=True)
    scores = scores * (HEAD**-0.5) + latest + log_gate - cum
    usable = position < used
    scores = jnp.where(usable, scores, MASKED_SCORE)
    own = jnp.sum(query_wide * key_new_ref[...], axis=1, keepdims=True) * (HEAD**-0.5)
    peak = jnp.maximum(jnp.max(scores, axis=1, keepdims=True), own)
    weights = jnp.where(usable, jnp.exp(scores - peak), 0.0)
    own_weight = jnp.exp(own - peak)
    denominator = jnp.sum(weights, axis=1, keepdims=True) + own_weight
    summed = jnp.dot(weights.astype(BF16), values_ref[0], preferred_element_type=F32)
    summed = summed + own_weight.astype(BF16).astype(F32) * value_new_ref[...]
    summed = jnp.where(in_block, summed, 0.0)
    summed = summed[:, : 2 * HEAD] + summed[:, 2 * HEAD :]
    summed = (summed[:, :HEAD] + summed[:, HEAD:]) / denominator
    both = jnp.concatenate([summed, summed], axis=1).astype(BF16)
    mine = index(both.shape, 1) // HEAD == index(both.shape, 0) % 2
    both = jnp.where(mine, both, jnp.zeros((), BF16))
    attended = jnp.dot(to_pairs, both, preferred_element_type=F32).astype(BF16)
    out_ref[...] = jnp.broadcast_to(attended[None], out_ref.shape)


def mix_kernel(place_ref, parts_ref, w_ref, tokens_ref, send_ref, mixed_ref, packed_ref, wide_ref):
    rows, chunks, lanes = parts_ref.shape
    wide_ref[...] = parts_ref[...].reshape(rows * chunks, lanes).astype(F32)
    attended = jnp.concatenate(
        [wide_ref[pl.ds(i, rows, stride=chunks), :].astype(BF16) for i in range(chunks)], axis=1
    )
    projected = jnp.dot(attended, w_ref[...], preferred_element_type=F32)
    first = pl.multiple_of(place_ref[0] * lanes, lanes)
    residual = tokens_ref[:, pl.ds(first, lanes)].astype(F32)
    mixed = (residual + projected).astype(BF16)
    mixed_ref[...] = mixed
    packed_ref[...] = jnp.dot(send_ref[...], mixed, preferred_element_type=F32).astype(BF16)


def hidden_kernel(parts_ref, gain_ref, w_gate_ref, w_up_ref, out_ref, inputs_ref):
    cores, chips, rows, lanes = parts_ref.shape
    squares = jnp.zeros((rows, lanes), F32)
    for core in range(cores):
        for chip in range(chips):
            part = parts_ref[core, chip].astype(F32)
            squares = squares + part * part
    mean = jnp.sum(squares, axis=-1, keepdims=True) / (cores * chips * lanes)
    scale = lax.rsqrt(mean + NORM_EPSILON)
    for core in range(cores):
        for chip in range(chips):
            first = (chip * cores + core) * lanes
            part = parts_ref[core, chip].astype(F32)
            gain = gain_ref[chip * cores + core : chip * cores + core + 1].astype(F32)
            inputs_ref[:, first : first + lanes] = (part * scale * gain).astype(BF16)
    inputs = inputs_ref[...]
    gate = jnp.dot(inputs, w_gate_ref[0], preferred_element_type=F32)
    up = jnp.dot(inputs, w_up_ref[0], preferred_element_type=F32)
    hidden = (gate / (1.0 + jnp.exp(-gate)) * up).astype(BF16)
    out_ref[...] = jnp.broadcast_to(hidden[None], out_ref.shape)


def down_kernel(parts_ref, w_ref, out_ref, hidden_ref):
    cores, chips, _, lanes = parts_ref.shape
    for core in range(cores):
        for chip in range(chips):
            first = (chip * cores + core) * lanes
            hidden_ref[:, first : first + lanes] = parts_ref[core, chip]
    out_ref[...] = jnp.dot(hidden_ref[...], w_ref[0], preferred_element_type=F32).astype(BF16)


def combine_kernel(returned_ref, combine_ref, mixed_ref, out_ref):
    returned = returned_ref[...]
    rest = combine_ref[...]
    total = jnp.zeros(out_ref.shape, F32)
    for _ in range(3):
        part = rest.astype(BF16)
        rest = rest - part.astype(F32)
        total = total + lax.dot_general(
            part, returned, (((0,), (0,)), ((), ())), preferred_element_type=F32
        )
    out_ref[...] = (mixed_ref[...].astype(F32) + total).astype(BF16)


def solution(mesh):
    experts = mesh.shape["ep"]
    peers = mesh.shape["tp"]
    chips = peers // CORES
    split = Mesh(mesh.devices.reshape(experts, chips, CORES), ("ep", "y", "core"))
    tp = ("y", "core")

    def to_all(copies):
        exchanged = lax.all_to_all(copies, "y", 0, 0, tiled=True)
        return lax.all_gather(exchanged, "core", axis=0, tiled=False)

    def on_device(
        tokens,
        attn_gain,
        ffn_gain,
        w_query,
        w_key,
        w_value,
        w_forget,
        forget_bias,
        w_out,
        cache_keys,
        cache_values,
        cache_logcum,
        cache_len,
        route_group,
        route_expert,
        route_weight,
        w_gate,
        w_up,
        w_down,
    ):
        rows, features = tokens.shape
        part = w_query.shape[1]
        slots = experts * TOP
        place = (lax.axis_index("y") * CORES + lax.axis_index("core")).astype(jnp.int32)
        place = place.reshape(1)
        normed, query = call(
            query_kernel,
            (shaped((rows, features), BF16), shaped((rows, part), BF16)),
            (tokens, attn_gain.reshape(peers, part), w_query),
            [VM] * 3,
            flops=20_000_000,
        )
        own_query = lax.all_to_all(
            query.reshape(peers, 1, part), tp, split_axis=0, concat_axis=0, tiled=True
        ).reshape(peers, part)

        def side(*refs):
            side_kernel(*refs, per_group=experts // GROUPS)

        kv = w_key.shape[1]
        key_new, value_new, log_gate, send, combine = call(
            side,
            (
                shaped((1, kv), F32),
                shaped((1, kv), F32),
                shaped((QUERY_HEAD_COUNT, 128), F32),
                shaped((slots, rows), BF16),
                shaped((slots, rows), F32),
            ),
            (
                place,
                normed,
                w_key,
                w_value,
                w_forget.T,
                forget_bias.reshape(1, QUERY_HEAD_COUNT),
                route_group.reshape(1, rows),
                route_expert.T,
                route_weight.T,
            ),
            [SM] + [VM] * 8,
            flops=2_000_000_000,
        )
        copies = call(
            attend_kernel,
            shaped((peers, peers, part), BF16),
            (cache_len, own_query, key_new, value_new, log_gate, cache_keys, cache_values, cache_logcum),
            [SM] + [VM] * 7,
            flops=200_000_000,
        )
        attended = lax.all_to_all(copies, tp, 0, 0, tiled=True)
        mixed, packed = call(
            mix_kernel,
            (shaped((rows, part), BF16), shaped((slots, part), BF16)),
            (place, attended, w_out, tokens, send),
            [SM] + [VM] * 4,
            scratch=[pltpu.VMEM((rows * peers, part), F32)],
            flops=20_000_000,
        )
        arrived = lax.all_to_all(packed.reshape(experts, TOP, part), "ep", 0, 0, tiled=True)
        arrived = arrived.reshape(slots, part)
        parts = to_all(jnp.broadcast_to(arrived[None], (chips, slots, part)))
        hidden = call(
            hidden_kernel,
            shaped((chips, slots, part), BF16),
            (parts, ffn_gain.reshape(peers, part), w_gate, w_up),
            [VM] * 4,
            scratch=[pltpu.VMEM((slots, features), BF16)],
            flops=100_000_000,
        )
        result = call(
            down_kernel,
            shaped((slots, part), BF16),
            (to_all(hidden), w_down),
            [VM] * 2,
            scratch=[pltpu.VMEM((slots, features), BF16)],
            flops=50_000_000,
        )
        returned = lax.all_to_all(result.reshape(experts, TOP, part), "ep", 0, 0, tiled=True)
        return call(
            combine_kernel,
            shaped((rows, part), BF16),
            (returned.reshape(slots, part), combine, mixed),
            [VM] * 3,
            flops=2_000_000,
        )

    placed = (
        P("ep", None),
        P(),
        P(),
        P(None, tp),
        P(),
        P(),
        P(),
        P(),
        P(None, tp),
        P(("ep", *tp), None, None),
        P(("ep", *tp), None, None),
        P(("ep", *tp), None, None),
        P(("ep", *tp)),
        P("ep"),
        P("ep", None),
        P("ep", None),
        P("ep", None, tp),
        P("ep", None, tp),
        P("ep", None, tp),
    )
    return jax.shard_map(
        on_device, mesh=split, in_specs=placed, out_specs=P("ep", tp), check_vma=False
    )
```

```python
import jax
import jax.numpy as jnp
from jax import lax
from jax.experimental import pallas as pl
from jax.experimental.pallas import tpu as pltpu
from jax.sharding import Mesh
from jax.sharding import PartitionSpec as P

QUERY_HEAD_COUNT = 32
KV_HEADS = 4
HEAD = 64
GROUPS = 4
TOP = 2
NORM_EPSILON = 1e-06
MASKED_SCORE = -1e30
CORES = 2
VMEM_LIMIT = 8 * 1024 * 1024
HEAD_LIMIT = 67_043_328 - 3072 * 1024

F32 = jnp.float32
BF16 = jnp.bfloat16
VM = pl.BlockSpec(memory_space=pltpu.VMEM)
HB = pl.BlockSpec(memory_space=pltpu.HBM)
SM = pl.BlockSpec(memory_space=pltpu.SMEM)


def call(body, outs, operands, specs, scratch=(), flops=1_000_000, moved=1_000_000, limit=VMEM_LIMIT):
    return pl.pallas_call(
        body,
        out_shape=outs,
        in_specs=specs,
        out_specs=jax.tree.map(lambda _: VM, outs),
        scratch_shapes=list(scratch),
        compiler_params=pltpu.CompilerParams(vmem_limit_bytes=limit),
        cost_estimate=pl.CostEstimate(flops=flops, bytes_accessed=moved, transcendentals=0),
    )(*operands)


def shaped(shape, dtype):
    return jax.ShapeDtypeStruct(shape, dtype)


def held(shape, dtype):
    return pltpu.VMEM(shape, dtype)


def head_kernel(
    place_ref,
    length_hbm,
    tokens_hbm,
    gain_hbm,
    w_query_hbm,
    w_key_hbm,
    w_value_hbm,
    w_forget_hbm,
    bias_hbm,
    group_hbm,
    expert_hbm,
    weight_hbm,
    query_ref,
    key_ref,
    value_ref,
    gate_ref,
    send_ref,
    combine_ref,
    used_ref,
    residual_ref,
    length_ref,
    tokens_ref,
    gain_ref,
    w_query_ref,
    w_key_ref,
    w_value_ref,
    w_forget_ref,
    bias_ref,
    group_ref,
    expert_ref,
    weight_ref,
    sems,
    *,
    per_group,
):
    sources = (
        tokens_hbm, gain_hbm, w_query_hbm, group_hbm, expert_hbm, weight_hbm, bias_hbm, w_forget_hbm,
        w_key_hbm, w_value_hbm, length_hbm,
    )
    targets = (
        tokens_ref, gain_ref, w_query_ref, group_ref, expert_ref, weight_ref, bias_ref, w_forget_ref,
        w_key_ref, w_value_ref, length_ref,
    )
    loads = [
        pltpu.make_async_copy(source, target, sems.at[i])
        for i, (source, target) in enumerate(zip(sources, targets))
    ]
    for load in loads:
        load.start()
    for load in loads[:2]:
        load.wait()
    place = place_ref[0]
    values = tokens_ref[...].astype(F32)
    rows = values.shape[0]
    mean = jnp.mean(values * values, axis=-1, keepdims=True)
    scaled = values * lax.rsqrt(mean + NORM_EPSILON)
    lanes = gain_ref.shape[1]
    normed = jnp.concatenate(
        [
            (scaled[:, i * lanes : (i + 1) * lanes] * gain_ref[i : i + 1].astype(F32)).astype(BF16)
            for i in range(gain_ref.shape[0])
        ],
        axis=1,
    )
    first = pl.multiple_of(place * lanes, lanes)
    residual_ref[...] = tokens_ref[:, pl.ds(first, lanes)]
    for load in loads[2:6]:
        load.wait()
    query_ref[...] = jnp.dot(normed, w_query_ref[...], preferred_element_type=F32).astype(BF16)

    picked = group_ref[...] * per_group + expert_ref[...]
    row_index = lax.broadcasted_iota(jnp.int32, (rows, rows), 0)
    column_index = lax.broadcasted_iota(jnp.int32, (rows, rows), 1)
    lines = [picked[j : j + 1] for j in range(TOP)]
    columns = [
        jnp.sum(jnp.where(row_index == column_index, line, 0), axis=1, keepdims=True)
        for line in lines
    ]
    slots, _ = send_ref.shape
    slot_index = lax.broadcasted_iota(jnp.int32, (slots, rows), 0)
    send = jnp.zeros((slots, rows), F32)
    combine = jnp.zeros((slots, rows), F32)
    for j in range(TOP):
        earlier = jnp.zeros((1, rows), jnp.int32)
        for other in columns:
            same = (other == lines[j]) & (row_index < column_index)
            earlier = earlier + jnp.sum(same.astype(jnp.int32), axis=0, keepdims=True)
        hit = slot_index == lines[j] * TOP + earlier
        send = send + jnp.where(hit, 1.0, 0.0)
        combine = combine + jnp.where(hit, weight_ref[j : j + 1], 0.0)
    send_ref[...] = send.astype(BF16)
    combine_ref[...] = combine

    for load in loads[6:8]:
        load.wait()
    logits = lax.dot_general(
        w_forget_ref[...], normed, (((1,), (1,)), ((), ())), preferred_element_type=F32
    )
    heads = QUERY_HEAD_COUNT
    own_column = lax.broadcasted_iota(jnp.int32, (1, rows), 1) == place
    logit = jnp.sum(jnp.where(own_column, logits, 0.0), axis=1, keepdims=True)
    diagonal = lax.broadcasted_iota(jnp.int32, (heads, heads), 0) == lax.broadcasted_iota(
        jnp.int32, (heads, heads), 1
    )
    bias = jnp.sum(jnp.where(diagonal, bias_ref[...], 0.0), axis=1, keepdims=True)
    logit = logit + bias
    log_gate = jnp.minimum(logit, 0.0) - jnp.log1p(jnp.exp(-jnp.abs(logit)))
    gate_ref[...] = jnp.broadcast_to(log_gate, gate_ref.shape)

    own_row = lax.broadcasted_iota(jnp.int32, (rows, 1), 0) == place

    def projected(w_ref):
        full = jnp.dot(normed, w_ref[...], preferred_element_type=F32)
        return jnp.sum(jnp.where(own_row, full, 0.0), axis=0, keepdims=True)

    loads[10].wait()
    used_ref[...] = jnp.broadcast_to(length_ref[...], used_ref.shape)
    loads[8].wait()
    key_ref[...] = projected(w_key_ref).astype(BF16).astype(F32)
    loads[9].wait()
    value_ref[...] = projected(w_value_ref).astype(BF16).astype(F32)


def attend_kernel(
    used_ref, query_ref, key_ref, value_ref, gate_ref, keys_ref, values_ref, cum_ref, out_ref
):
    heads = QUERY_HEAD_COUNT
    pairs = heads // 2
    width = KV_HEADS * HEAD
    used = used_ref[:1, :1]

    def index(shape, dim):
        return lax.broadcasted_iota(jnp.int32, shape, dim)

    to_heads = (index((heads, pairs), 0) // 2 == index((heads, pairs), 1)).astype(BF16)
    to_pairs = (index((pairs, heads), 1) // 2 == index((pairs, heads), 0)).astype(BF16)
    doubled = jnp.dot(to_heads, query_ref[...], preferred_element_type=F32)
    odd_row = index((heads, HEAD), 0) % 2 == 1
    one_head = jnp.where(odd_row, doubled[:, HEAD:], doubled[:, :HEAD])
    in_block = index((heads, width), 1) // HEAD == index((heads, width), 0) // (heads // KV_HEADS)
    query_wide = jnp.where(in_block, jnp.concatenate([one_head] * KV_HEADS, axis=1), 0.0)
    query_all = query_wide.astype(BF16)
    scores = lax.dot_general(
        query_all, keys_ref[0], (((1,), (1,)), ((), ())), preferred_element_type=F32
    )
    cum = cum_ref[0]
    log_gate = gate_ref[:, :1]
    position = lax.broadcasted_iota(jnp.int32, scores.shape, 1)
    latest = jnp.sum(jnp.where(position == used - 1, cum, 0.0), axis=1, keepdims=True)
    scores = scores * (HEAD**-0.5) + latest + log_gate - cum
    usable = position < used
    scores = jnp.where(usable, scores, MASKED_SCORE)
    own = jnp.sum(query_wide * key_ref[...], axis=1, keepdims=True) * (HEAD**-0.5)
    peak = jnp.maximum(jnp.max(scores, axis=1, keepdims=True), own)
    weights = jnp.where(usable, jnp.exp(scores - peak), 0.0)
    own_weight = jnp.exp(own - peak)
    denominator = jnp.sum(weights, axis=1, keepdims=True) + own_weight
    summed = jnp.dot(weights.astype(BF16), values_ref[0], preferred_element_type=F32)
    summed = summed + own_weight.astype(BF16).astype(F32) * value_ref[...]
    summed = jnp.where(in_block, summed, 0.0)
    summed = summed[:, : 2 * HEAD] + summed[:, 2 * HEAD :]
    summed = (summed[:, :HEAD] + summed[:, HEAD:]) / denominator
    both = jnp.concatenate([summed, summed], axis=1).astype(BF16)
    mine = index(both.shape, 1) // HEAD == index(both.shape, 0) % 2
    both = jnp.where(mine, both, jnp.zeros((), BF16))
    attended = jnp.dot(to_pairs, both, preferred_element_type=F32).astype(BF16)
    out_ref[...] = jnp.broadcast_to(attended[None], out_ref.shape)


def mix_kernel(parts_ref, w_ref, residual_ref, send_ref, mixed_ref, packed_ref, wide_ref):
    rows, chunks, lanes = parts_ref.shape
    wide_ref[...] = parts_ref[...].reshape(rows * chunks, lanes).astype(F32)
    attended = jnp.concatenate(
        [wide_ref[pl.ds(i, rows, stride=chunks), :].astype(BF16) for i in range(chunks)], axis=1
    )
    projected = jnp.dot(attended, w_ref[...], preferred_element_type=F32)
    mixed = (residual_ref[...].astype(F32) + projected).astype(BF16)
    mixed_ref[...] = mixed
    packed_ref[...] = jnp.dot(send_ref[...], mixed, preferred_element_type=F32).astype(BF16)


def hidden_kernel(parts_ref, gain_ref, w_gate_ref, w_up_ref, out_ref, inputs_ref):
    cores, chips, rows, lanes = parts_ref.shape
    squares = jnp.zeros((rows, lanes), F32)
    for core in range(cores):
        for chip in range(chips):
            part = parts_ref[core, chip].astype(F32)
            squares = squares + part * part
    mean = jnp.sum(squares, axis=-1, keepdims=True) / (cores * chips * lanes)
    scale = lax.rsqrt(mean + NORM_EPSILON)
    for core in range(cores):
        for chip in range(chips):
            first = (chip * cores + core) * lanes
            part = parts_ref[core, chip].astype(F32)
            gain = gain_ref[chip * cores + core : chip * cores + core + 1].astype(F32)
            inputs_ref[:, first : first + lanes] = (part * scale * gain).astype(BF16)
    inputs = inputs_ref[...]
    gate = jnp.dot(inputs, w_gate_ref[0], preferred_element_type=F32)
    up = jnp.dot(inputs, w_up_ref[0], preferred_element_type=F32)
    hidden = (gate / (1.0 + jnp.exp(-gate)) * up).astype(BF16)
    out_ref[...] = jnp.broadcast_to(hidden[None], out_ref.shape)


def down_kernel(parts_ref, w_ref, out_ref, hidden_ref):
    cores, chips, _, lanes = parts_ref.shape
    for core in range(cores):
        for chip in range(chips):
            first = (chip * cores + core) * lanes
            hidden_ref[:, first : first + lanes] = parts_ref[core, chip]
    out_ref[...] = jnp.dot(hidden_ref[...], w_ref[0], preferred_element_type=F32).astype(BF16)


def combine_kernel(returned_ref, combine_ref, mixed_ref, out_ref):
    returned = returned_ref[...]
    rest = combine_ref[...]
    total = jnp.zeros(out_ref.shape, F32)
    for _ in range(3):
        part = rest.astype(BF16)
        rest = rest - part.astype(F32)
        total = total + lax.dot_general(
            part, returned, (((0,), (0,)), ((), ())), preferred_element_type=F32
        )
    out_ref[...] = (mixed_ref[...].astype(F32) + total).astype(BF16)


def solution(mesh):
    experts = mesh.shape["ep"]
    peers = mesh.shape["tp"]
    chips = peers // CORES
    split = Mesh(mesh.devices.reshape(experts, chips, CORES), ("ep", "y", "core"))
    tp = ("y", "core")

    def to_all(copies):
        exchanged = lax.all_to_all(copies, "y", 0, 0, tiled=True)
        return lax.all_gather(exchanged, "core", axis=0, tiled=False)

    def on_device(
        tokens,
        attn_gain,
        ffn_gain,
        w_query,
        w_key,
        w_value,
        w_forget,
        forget_bias,
        w_out,
        cache_keys,
        cache_values,
        cache_logcum,
        cache_len,
        route_group,
        route_expert,
        route_weight,
        w_gate,
        w_up,
        w_down,
    ):
        rows, features = tokens.shape
        part = w_query.shape[1]
        slots = experts * TOP
        place = (lax.axis_index("y") * CORES + lax.axis_index("core")).astype(jnp.int32)
        place = place.reshape(1)
        def head(*refs):
            head_kernel(*refs, per_group=experts // GROUPS)

        kv = w_key.shape[1]
        operands = (
            cache_len.reshape(1, 1),
            tokens,
            attn_gain.reshape(peers, part),
            w_query,
            w_key,
            w_value,
            w_forget.T,
            forget_bias.reshape(1, QUERY_HEAD_COUNT),
            route_group.reshape(1, rows),
            route_expert.T,
            route_weight.T,
        )
        query, key_new, value_new, log_gate, send, combine, used, residual = call(
            head,
            (
                held((rows, part), BF16),
                held((1, kv), F32),
                held((1, kv), F32),
                held((QUERY_HEAD_COUNT, 128), F32),
                held((slots, rows), BF16),
                held((slots, rows), F32),
                held((8, 128), jnp.int32),
                held((rows, part), BF16),
            ),
            (place, *operands),
            [SM] + [HB] * len(operands),
            scratch=[pltpu.VMEM(one.shape, one.dtype) for one in operands]
            + [pltpu.SemaphoreType.DMA((len(operands),))],
            flops=50_000_000,
            limit=HEAD_LIMIT,
        )
        own_query = lax.all_to_all(
            query.reshape(peers, 1, part), tp, split_axis=0, concat_axis=0, tiled=True
        ).reshape(peers, part)
        copies = call(
            attend_kernel,
            shaped((peers, peers, part), BF16),
            (used, own_query, key_new, value_new, log_gate, cache_keys, cache_values, cache_logcum),
            [VM] * 8,
            flops=200_000_000,
        )
        attended = lax.all_to_all(copies, tp, 0, 0, tiled=True)
        mixed, packed = call(
            mix_kernel,
            (shaped((rows, part), BF16), shaped((slots, part), BF16)),
            (attended, w_out, residual, send),
            [VM] * 4,
            scratch=[pltpu.VMEM((rows * peers, part), F32)],
            flops=20_000_000,
        )
        arrived = lax.all_to_all(packed.reshape(experts, TOP, part), "ep", 0, 0, tiled=True)
        arrived = arrived.reshape(slots, part)
        parts = to_all(jnp.broadcast_to(arrived[None], (chips, slots, part)))
        hidden = call(
            hidden_kernel,
            shaped((chips, slots, part), BF16),
            (parts, ffn_gain.reshape(peers, part), w_gate, w_up),
            [VM] * 4,
            scratch=[pltpu.VMEM((slots, features), BF16)],
            flops=100_000_000,
        )
        result = call(
            down_kernel,
            shaped((slots, part), BF16),
            (to_all(hidden), w_down),
            [VM] * 2,
            scratch=[pltpu.VMEM((slots, features), BF16)],
            flops=50_000_000,
        )
        returned = lax.all_to_all(result.reshape(experts, TOP, part), "ep", 0, 0, tiled=True)
        return call(
            combine_kernel,
            shaped((rows, part), BF16),
            (returned.reshape(slots, part), combine, mixed),
            [VM] * 3,
            flops=2_000_000,
        )

    placed = (
        P("ep", None),
        P(),
        P(),
        P(None, tp),
        P(),
        P(),
        P(),
        P(),
        P(None, tp),
        P(("ep", *tp), None, None),
        P(("ep", *tp), None, None),
        P(("ep", *tp), None, None),
        P(("ep", *tp)),
        P("ep"),
        P("ep", None),
        P("ep", None),
        P("ep", None, tp),
        P("ep", None, tp),
        P("ep", None, tp),
    )
    return jax.shard_map(
        on_device, mesh=split, in_specs=placed, out_specs=P("ep", tp), check_vma=False
    )
```

```python
import jax
import jax.numpy as jnp
from jax import lax
from jax.experimental import pallas as pl
from jax.experimental.pallas import tpu as pltpu
from jax.sharding import Mesh
from jax.sharding import PartitionSpec as P

QUERY_HEAD_COUNT = 32
KV_HEADS = 4
HEAD = 64
GROUPS = 4
TOP = 2
NORM_EPSILON = 1e-06
MASKED_SCORE = -1e30
CORES = 2
VMEM_LIMIT = 8 * 1024 * 1024
HEAD_LIMIT = 67_043_328 - 512 * 1024

F32 = jnp.float32
BF16 = jnp.bfloat16
VM = pl.BlockSpec(memory_space=pltpu.VMEM)
HB = pl.BlockSpec(memory_space=pltpu.HBM)
SM = pl.BlockSpec(memory_space=pltpu.SMEM)


def call(body, outs, operands, specs, scratch=(), flops=1_000_000, moved=1_000_000, limit=VMEM_LIMIT):
    return pl.pallas_call(
        body,
        out_shape=outs,
        in_specs=specs,
        out_specs=jax.tree.map(lambda _: VM, outs),
        scratch_shapes=list(scratch),
        compiler_params=pltpu.CompilerParams(vmem_limit_bytes=limit),
        cost_estimate=pl.CostEstimate(flops=flops, bytes_accessed=moved, transcendentals=0),
    )(*operands)


def shaped(shape, dtype):
    return jax.ShapeDtypeStruct(shape, dtype)


def held(shape, dtype):
    return pltpu.VMEM(shape, dtype)


def head_kernel(
    place_ref,
    length_hbm,
    tokens_hbm,
    gain_hbm,
    w_query_hbm,
    bias_hbm,
    group_hbm,
    expert_hbm,
    weight_hbm,
    query_ref,
    normed_ref,
    bias_out_ref,
    send_ref,
    combine_ref,
    used_ref,
    residual_ref,
    length_ref,
    tokens_ref,
    gain_ref,
    w_query_ref,
    bias_ref,
    group_ref,
    expert_ref,
    weight_ref,
    sems,
    *,
    per_group,
):
    sources = (
        tokens_hbm, gain_hbm, w_query_hbm, group_hbm, expert_hbm, weight_hbm, bias_hbm, length_hbm
    )
    targets = (
        tokens_ref, gain_ref, w_query_ref, group_ref, expert_ref, weight_ref, bias_ref, length_ref
    )
    loads = [
        pltpu.make_async_copy(source, target, sems.at[i])
        for i, (source, target) in enumerate(zip(sources, targets))
    ]
    for load in loads:
        load.start()
    for load in loads[:2]:
        load.wait()
    values = tokens_ref[...].astype(F32)
    rows = values.shape[0]
    mean = jnp.mean(values * values, axis=-1, keepdims=True)
    scaled = values * lax.rsqrt(mean + NORM_EPSILON)
    lanes = gain_ref.shape[1]
    normed = jnp.concatenate(
        [
            (scaled[:, i * lanes : (i + 1) * lanes] * gain_ref[i : i + 1].astype(F32)).astype(BF16)
            for i in range(gain_ref.shape[0])
        ],
        axis=1,
    )
    normed_ref[...] = normed
    first = pl.multiple_of(place_ref[0] * lanes, lanes)
    residual_ref[...] = tokens_ref[:, pl.ds(first, lanes)]
    for load in loads[2:]:
        load.wait()
    query_ref[...] = jnp.dot(normed, w_query_ref[...], preferred_element_type=F32).astype(BF16)

    picked = group_ref[...] * per_group + expert_ref[...]
    row_index = lax.broadcasted_iota(jnp.int32, (rows, rows), 0)
    column_index = lax.broadcasted_iota(jnp.int32, (rows, rows), 1)
    lines = [picked[j : j + 1] for j in range(TOP)]
    columns = [
        jnp.sum(jnp.where(row_index == column_index, line, 0), axis=1, keepdims=True)
        for line in lines
    ]
    slots, _ = send_ref.shape
    slot_index = lax.broadcasted_iota(jnp.int32, (slots, rows), 0)
    send = jnp.zeros((slots, rows), F32)
    combine = jnp.zeros((slots, rows), F32)
    for j in range(TOP):
        earlier = jnp.zeros((1, rows), jnp.int32)
        for other in columns:
            same = (other == lines[j]) & (row_index < column_index)
            earlier = earlier + jnp.sum(same.astype(jnp.int32), axis=0, keepdims=True)
        hit = slot_index == lines[j] * TOP + earlier
        send = send + jnp.where(hit, 1.0, 0.0)
        combine = combine + jnp.where(hit, weight_ref[j : j + 1], 0.0)
    send_ref[...] = send.astype(BF16)
    combine_ref[...] = combine

    heads = QUERY_HEAD_COUNT
    diagonal = lax.broadcasted_iota(jnp.int32, (heads, heads), 0) == lax.broadcasted_iota(
        jnp.int32, (heads, heads), 1
    )
    bias = jnp.sum(jnp.where(diagonal, bias_ref[...], 0.0), axis=1, keepdims=True)
    bias_out_ref[...] = jnp.broadcast_to(bias, bias_out_ref.shape)
    used_ref[...] = jnp.broadcast_to(length_ref[...], used_ref.shape)


def pass_kernel(query_ref, out_ref):
    out_ref[...] = query_ref[...]


def attend_kernel(
    place_ref,
    used_ref,
    query_ref,
    normed_ref,
    w_key_ref,
    w_value_ref,
    w_forget_ref,
    bias_ref,
    keys_ref,
    values_ref,
    cum_ref,
    out_ref,
):
    place = place_ref[0]
    normed = normed_ref[...]
    rows = normed.shape[0]
    own_row = lax.broadcasted_iota(jnp.int32, (rows, 1), 0) == place
    own_column = lax.broadcasted_iota(jnp.int32, (1, rows), 1) == place

    def projected(w_ref):
        full = jnp.dot(normed, w_ref[...], preferred_element_type=F32)
        one = jnp.sum(jnp.where(own_row, full, 0.0), axis=0, keepdims=True)
        return one.astype(BF16).astype(F32)

    key_new = projected(w_key_ref)
    value_new = projected(w_value_ref)
    logits = lax.dot_general(
        w_forget_ref[...], normed, (((1,), (1,)), ((), ())), preferred_element_type=F32
    )
    logit = jnp.sum(jnp.where(own_column, logits, 0.0), axis=1, keepdims=True) + bias_ref[:, :1]
    log_gate = jnp.minimum(logit, 0.0) - jnp.log1p(jnp.exp(-jnp.abs(logit)))
    heads = QUERY_HEAD_COUNT
    pairs = heads // 2
    width = KV_HEADS * HEAD
    used = used_ref[:1, :1]

    def index(shape, dim):
        return lax.broadcasted_iota(jnp.int32, shape, dim)

    to_heads = (index((heads, pairs), 0) // 2 == index((heads, pairs), 1)).astype(BF16)
    to_pairs = (index((pairs, heads), 1) // 2 == index((pairs, heads), 0)).astype(BF16)
    doubled = jnp.dot(to_heads, query_ref[...], preferred_element_type=F32)
    odd_row = index((heads, HEAD), 0) % 2 == 1
    one_head = jnp.where(odd_row, doubled[:, HEAD:], doubled[:, :HEAD])
    in_block = index((heads, width), 1) // HEAD == index((heads, width), 0) // (heads // KV_HEADS)
    query_wide = jnp.where(in_block, jnp.concatenate([one_head] * KV_HEADS, axis=1), 0.0)
    query_all = query_wide.astype(BF16)
    scores = lax.dot_general(
        query_all, keys_ref[0], (((1,), (1,)), ((), ())), preferred_element_type=F32
    )
    cum = cum_ref[0]
    position = lax.broadcasted_iota(jnp.int32, scores.shape, 1)
    latest = jnp.sum(jnp.where(position == used - 1, cum, 0.0), axis=1, keepdims=True)
    scores = scores * (HEAD**-0.5) + latest + log_gate - cum
    usable = position < used
    scores = jnp.where(usable, scores, MASKED_SCORE)
    own = jnp.sum(query_wide * key_new, axis=1, keepdims=True) * (HEAD**-0.5)
    peak = jnp.maximum(jnp.max(scores, axis=1, keepdims=True), own)
    weights = jnp.where(usable, jnp.exp(scores - peak), 0.0)
    own_weight = jnp.exp(own - peak)
    denominator = jnp.sum(weights, axis=1, keepdims=True) + own_weight
    summed = jnp.dot(weights.astype(BF16), values_ref[0], preferred_element_type=F32)
    summed = summed + own_weight.astype(BF16).astype(F32) * value_new
    summed = jnp.where(in_block, summed, 0.0)
    summed = summed[:, : 2 * HEAD] + summed[:, 2 * HEAD :]
    summed = (summed[:, :HEAD] + summed[:, HEAD:]) / denominator
    both = jnp.concatenate([summed, summed], axis=1).astype(BF16)
    mine = index(both.shape, 1) // HEAD == index(both.shape, 0) % 2
    both = jnp.where(mine, both, jnp.zeros((), BF16))
    attended = jnp.dot(to_pairs, both, preferred_element_type=F32).astype(BF16)
    out_ref[...] = jnp.broadcast_to(attended[None], out_ref.shape)


def mix_kernel(parts_ref, w_ref, residual_ref, send_ref, mixed_ref, packed_ref, wide_ref):
    rows, chunks, lanes = parts_ref.shape
    wide_ref[...] = parts_ref[...].reshape(rows * chunks, lanes).astype(F32)
    attended = jnp.concatenate(
        [wide_ref[pl.ds(i, rows, stride=chunks), :].astype(BF16) for i in range(chunks)], axis=1
    )
    projected = jnp.dot(attended, w_ref[...], preferred_element_type=F32)
    mixed = (residual_ref[...].astype(F32) + projected).astype(BF16)
    mixed_ref[...] = mixed
    packed_ref[...] = jnp.dot(send_ref[...], mixed, preferred_element_type=F32).astype(BF16)


def hidden_kernel(parts_ref, gain_ref, w_gate_ref, w_up_ref, out_ref, inputs_ref):
    cores, chips, rows, lanes = parts_ref.shape
    squares = jnp.zeros((rows, lanes), F32)
    for core in range(cores):
        for chip in range(chips):
            part = parts_ref[core, chip].astype(F32)
            squares = squares + part * part
    mean = jnp.sum(squares, axis=-1, keepdims=True) / (cores * chips * lanes)
    scale = lax.rsqrt(mean + NORM_EPSILON)
    for core in range(cores):
        for chip in range(chips):
            first = (chip * cores + core) * lanes
            part = parts_ref[core, chip].astype(F32)
            gain = gain_ref[chip * cores + core : chip * cores + core + 1].astype(F32)
            inputs_ref[:, first : first + lanes] = (part * scale * gain).astype(BF16)
    inputs = inputs_ref[...]
    gate = jnp.dot(inputs, w_gate_ref[0], preferred_element_type=F32)
    up = jnp.dot(inputs, w_up_ref[0], preferred_element_type=F32)
    hidden = (gate / (1.0 + jnp.exp(-gate)) * up).astype(BF16)
    out_ref[...] = jnp.broadcast_to(hidden[None], out_ref.shape)


def down_kernel(parts_ref, w_ref, out_ref, hidden_ref):
    cores, chips, _, lanes = parts_ref.shape
    for core in range(cores):
        for chip in range(chips):
            first = (chip * cores + core) * lanes
            hidden_ref[:, first : first + lanes] = parts_ref[core, chip]
    out_ref[...] = jnp.dot(hidden_ref[...], w_ref[0], preferred_element_type=F32).astype(BF16)


def combine_kernel(returned_ref, combine_ref, mixed_ref, out_ref):
    returned = returned_ref[...]
    rest = combine_ref[...]
    total = jnp.zeros(out_ref.shape, F32)
    for _ in range(3):
        part = rest.astype(BF16)
        rest = rest - part.astype(F32)
        total = total + lax.dot_general(
            part, returned, (((0,), (0,)), ((), ())), preferred_element_type=F32
        )
    out_ref[...] = (mixed_ref[...].astype(F32) + total).astype(BF16)


def solution(mesh):
    experts = mesh.shape["ep"]
    peers = mesh.shape["tp"]
    chips = peers // CORES
    split = Mesh(mesh.devices.reshape(experts, chips, CORES), ("ep", "y", "core"))
    tp = ("y", "core")

    def to_all(copies):
        exchanged = lax.all_to_all(copies, "y", 0, 0, tiled=True)
        return lax.all_gather(exchanged, "core", axis=0, tiled=False)

    def on_device(
        tokens,
        attn_gain,
        ffn_gain,
        w_query,
        w_key,
        w_value,
        w_forget,
        forget_bias,
        w_out,
        cache_keys,
        cache_values,
        cache_logcum,
        cache_len,
        route_group,
        route_expert,
        route_weight,
        w_gate,
        w_up,
        w_down,
    ):
        rows, features = tokens.shape
        part = w_query.shape[1]
        slots = experts * TOP
        place = (lax.axis_index("y") * CORES + lax.axis_index("core")).astype(jnp.int32)
        place = place.reshape(1)
        def head(*refs):
            head_kernel(*refs, per_group=experts // GROUPS)

        operands = (
            cache_len.reshape(1, 1),
            tokens,
            attn_gain.reshape(peers, part),
            w_query,
            forget_bias.reshape(1, QUERY_HEAD_COUNT),
            route_group.reshape(1, rows),
            route_expert.T,
            route_weight.T,
        )
        query, normed, bias, send, combine, used, residual = call(
            head,
            (
                held((rows, part), BF16),
                held((rows, features), BF16),
                held((QUERY_HEAD_COUNT, 128), F32),
                held((slots, rows), BF16),
                held((slots, rows), F32),
                held((8, 128), jnp.int32),
                held((rows, part), BF16),
            ),
            (place, *operands),
            [SM] + [HB] * len(operands),
            scratch=[pltpu.VMEM(one.shape, one.dtype) for one in operands]
            + [pltpu.SemaphoreType.DMA((len(operands),))],
            flops=10_000_000,
            limit=HEAD_LIMIT,
        )
        query = call(
            pass_kernel,
            held((rows, part), BF16),
            (query,),
            [VM],
            flops=20_000_000_000,
        )
        own_query = lax.all_to_all(
            query.reshape(peers, 1, part), tp, split_axis=0, concat_axis=0, tiled=True
        ).reshape(peers, part)
        copies = call(
            attend_kernel,
            shaped((peers, peers, part), BF16),
            (
                place,
                used,
                own_query,
                normed,
                w_key,
                w_value,
                w_forget.T,
                bias,
                cache_keys,
                cache_values,
                cache_logcum,
            ),
            [SM] + [VM] * 10,
            flops=200_000_000,
        )
        attended = lax.all_to_all(copies, tp, 0, 0, tiled=True)
        mixed, packed = call(
            mix_kernel,
            (shaped((rows, part), BF16), shaped((slots, part), BF16)),
            (attended, w_out, residual, send),
            [VM] * 4,
            scratch=[pltpu.VMEM((rows * peers, part), F32)],
            flops=20_000_000,
        )
        arrived = lax.all_to_all(packed.reshape(experts, TOP, part), "ep", 0, 0, tiled=True)
        arrived = arrived.reshape(slots, part)
        parts = to_all(jnp.broadcast_to(arrived[None], (chips, slots, part)))
        hidden = call(
            hidden_kernel,
            shaped((chips, slots, part), BF16),
            (parts, ffn_gain.reshape(peers, part), w_gate, w_up),
            [VM] * 4,
            scratch=[pltpu.VMEM((slots, features), BF16)],
            flops=100_000_000,
        )
        result = call(
            down_kernel,
            shaped((slots, part), BF16),
            (to_all(hidden), w_down),
            [VM] * 2,
            scratch=[pltpu.VMEM((slots, features), BF16)],
            flops=50_000_000,
        )
        returned = lax.all_to_all(result.reshape(experts, TOP, part), "ep", 0, 0, tiled=True)
        return call(
            combine_kernel,
            shaped((rows, part), BF16),
            (returned.reshape(slots, part), combine, mixed),
            [VM] * 3,
            flops=2_000_000,
        )

    placed = (
        P("ep", None),
        P(),
        P(),
        P(None, tp),
        P(),
        P(),
        P(),
        P(),
        P(None, tp),
        P(("ep", *tp), None, None),
        P(("ep", *tp), None, None),
        P(("ep", *tp), None, None),
        P(("ep", *tp)),
        P("ep"),
        P("ep", None),
        P("ep", None),
        P("ep", None, tp),
        P("ep", None, tp),
        P("ep", None, tp),
    )
    return jax.shard_map(
        on_device, mesh=split, in_specs=placed, out_specs=P("ep", tp), check_vma=False
    )
```

```python
import jax
import jax.numpy as jnp
from jax import lax
from jax.experimental import pallas as pl
from jax.experimental.pallas import tpu as pltpu
from jax.sharding import Mesh
from jax.sharding import PartitionSpec as P

QUERY_HEAD_COUNT = 32
KV_HEADS = 4
HEAD = 64
GROUPS = 4
TOP = 2
NORM_EPSILON = 1e-06
MASKED_SCORE = -1e30
CORES = 2
VMEM_LIMIT = 8 * 1024 * 1024
HEAD_LIMIT = 67_043_328 - 512 * 1024

F32 = jnp.float32
BF16 = jnp.bfloat16
VM = pl.BlockSpec(memory_space=pltpu.VMEM)
HB = pl.BlockSpec(memory_space=pltpu.HBM)


def call(body, outs, operands, specs, scratch=(), flops=1_000_000, moved=1_000_000, limit=VMEM_LIMIT):
    return pl.pallas_call(
        body,
        out_shape=outs,
        in_specs=specs,
        out_specs=jax.tree.map(lambda _: VM, outs),
        scratch_shapes=list(scratch),
        compiler_params=pltpu.CompilerParams(vmem_limit_bytes=limit),
        cost_estimate=pl.CostEstimate(flops=flops, bytes_accessed=moved, transcendentals=0),
    )(*operands)


def shaped(shape, dtype):
    return jax.ShapeDtypeStruct(shape, dtype)


def own_place():
    return lax.axis_index("y") * CORES + lax.axis_index("core")


def held(shape, dtype):
    return pltpu.VMEM(shape, dtype)


def head_kernel(
    length_hbm,
    tokens_hbm,
    gain_hbm,
    w_query_hbm,
    bias_hbm,
    group_hbm,
    expert_hbm,
    weight_hbm,
    query_ref,
    normed_ref,
    bias_out_ref,
    send_ref,
    combine_ref,
    used_ref,
    residual_ref,
    length_ref,
    tokens_ref,
    gain_ref,
    w_query_ref,
    bias_ref,
    group_ref,
    expert_ref,
    weight_ref,
    sems,
    *,
    per_group,
):
    sources = (
        tokens_hbm, gain_hbm, w_query_hbm, group_hbm, expert_hbm, weight_hbm, bias_hbm, length_hbm
    )
    targets = (
        tokens_ref, gain_ref, w_query_ref, group_ref, expert_ref, weight_ref, bias_ref, length_ref
    )
    loads = [
        pltpu.make_async_copy(source, target, sems.at[i])
        for i, (source, target) in enumerate(zip(sources, targets))
    ]
    for load in loads:
        load.start()
    for load in loads[:2]:
        load.wait()
    values = tokens_ref[...].astype(F32)
    rows = values.shape[0]
    mean = jnp.mean(values * values, axis=-1, keepdims=True)
    scaled = values * lax.rsqrt(mean + NORM_EPSILON)
    lanes = gain_ref.shape[1]
    normed = jnp.concatenate(
        [
            (scaled[:, i * lanes : (i + 1) * lanes] * gain_ref[i : i + 1].astype(F32)).astype(BF16)
            for i in range(gain_ref.shape[0])
        ],
        axis=1,
    )
    normed_ref[...] = normed
    place = own_place()
    first = pl.multiple_of(place * lanes, lanes)
    residual_ref[...] = tokens_ref[:, pl.ds(first, lanes)]
    for load in loads[2:]:
        load.wait()
    query_ref[...] = jnp.dot(normed, w_query_ref[...], preferred_element_type=F32).astype(BF16)

    picked = group_ref[...] * per_group + expert_ref[...]
    row_index = lax.broadcasted_iota(jnp.int32, (rows, rows), 0)
    column_index = lax.broadcasted_iota(jnp.int32, (rows, rows), 1)
    lines = [picked[j : j + 1] for j in range(TOP)]
    columns = [
        jnp.sum(jnp.where(row_index == column_index, line, 0), axis=1, keepdims=True)
        for line in lines
    ]
    slots, _ = send_ref.shape
    slot_index = lax.broadcasted_iota(jnp.int32, (slots, rows), 0)
    send = jnp.zeros((slots, rows), F32)
    combine = jnp.zeros((slots, rows), F32)
    for j in range(TOP):
        earlier = jnp.zeros((1, rows), jnp.int32)
        for other in columns:
            same = (other == lines[j]) & (row_index < column_index)
            earlier = earlier + jnp.sum(same.astype(jnp.int32), axis=0, keepdims=True)
        hit = slot_index == lines[j] * TOP + earlier
        send = send + jnp.where(hit, 1.0, 0.0)
        combine = combine + jnp.where(hit, weight_ref[j : j + 1], 0.0)
    send_ref[...] = send.astype(BF16)
    combine_ref[...] = combine

    heads = QUERY_HEAD_COUNT
    diagonal = lax.broadcasted_iota(jnp.int32, (heads, heads), 0) == lax.broadcasted_iota(
        jnp.int32, (heads, heads), 1
    )
    bias = jnp.sum(jnp.where(diagonal, bias_ref[...], 0.0), axis=1, keepdims=True)
    bias_out_ref[...] = jnp.broadcast_to(bias, bias_out_ref.shape)
    used_ref[...] = jnp.broadcast_to(length_ref[...], used_ref.shape)


def pass_kernel(query_ref, out_ref):
    out_ref[...] = query_ref[...]


def attend_kernel(
    used_ref,
    query_ref,
    normed_ref,
    w_key_ref,
    w_value_ref,
    w_forget_ref,
    bias_ref,
    keys_ref,
    values_ref,
    cum_ref,
    out_ref,
    rows_ref,
):
    place = own_place()
    normed = normed_ref[...]
    rows = normed.shape[0]
    own_row = lax.broadcasted_iota(jnp.int32, (rows, 1), 0) == place
    own_column = lax.broadcasted_iota(jnp.int32, (1, rows), 1) == place

    def projected(w_ref):
        full = jnp.dot(normed, w_ref[...], preferred_element_type=F32)
        one = jnp.sum(jnp.where(own_row, full, 0.0), axis=0, keepdims=True)
        return one.astype(BF16).astype(F32)

    key_new = projected(w_key_ref)
    value_new = projected(w_value_ref)
    logits = lax.dot_general(
        w_forget_ref[...], normed, (((1,), (1,)), ((), ())), preferred_element_type=F32
    )
    logit = jnp.sum(jnp.where(own_column, logits, 0.0), axis=1, keepdims=True) + bias_ref[:, :1]
    log_gate = jnp.minimum(logit, 0.0) - jnp.log1p(jnp.exp(-jnp.abs(logit)))
    heads = QUERY_HEAD_COUNT
    pairs = heads // 2
    width = KV_HEADS * HEAD
    used = used_ref[:1, :1]

    def index(shape, dim):
        return lax.broadcasted_iota(jnp.int32, shape, dim)

    query = query_ref[...].astype(F32)
    rows_ref[pl.ds(0, pairs, stride=2), :] = query
    rows_ref[pl.ds(1, pairs, stride=2), :] = query
    doubled = rows_ref[...]
    odd_row = index((heads, HEAD), 0) % 2 == 1
    one_head = jnp.where(odd_row, doubled[:, HEAD:], doubled[:, :HEAD])
    in_block = index((heads, width), 1) // HEAD == index((heads, width), 0) // (heads // KV_HEADS)
    query_wide = jnp.where(in_block, jnp.concatenate([one_head] * KV_HEADS, axis=1), 0.0)
    query_all = query_wide.astype(BF16)
    scores = lax.dot_general(
        query_all, keys_ref[0], (((1,), (1,)), ((), ())), preferred_element_type=F32
    )
    cum = cum_ref[0]
    position = lax.broadcasted_iota(jnp.int32, scores.shape, 1)
    latest = jnp.sum(jnp.where(position == used - 1, cum, 0.0), axis=1, keepdims=True)
    scores = scores * (HEAD**-0.5) + latest + log_gate - cum
    usable = position < used
    scores = jnp.where(usable, scores, MASKED_SCORE)
    own = jnp.sum(query_wide * key_new, axis=1, keepdims=True) * (HEAD**-0.5)
    peak = jnp.maximum(jnp.max(scores, axis=1, keepdims=True), own)
    weights = jnp.where(usable, jnp.exp(scores - peak), 0.0)
    own_weight = jnp.exp(own - peak)
    denominator = jnp.sum(weights, axis=1, keepdims=True) + own_weight
    summed = jnp.dot(weights.astype(BF16), values_ref[0], preferred_element_type=F32)
    summed = summed + own_weight.astype(BF16).astype(F32) * value_new
    summed = jnp.where(in_block, summed, 0.0)
    summed = summed[:, : 2 * HEAD] + summed[:, 2 * HEAD :]
    summed = (summed[:, :HEAD] + summed[:, HEAD:]) / denominator
    rows_ref[...] = jnp.concatenate([summed, summed], axis=1)
    even = rows_ref[pl.ds(0, pairs, stride=2), :]
    odd = rows_ref[pl.ds(1, pairs, stride=2), :]
    attended = jnp.where(index((pairs, 2 * HEAD), 1) < HEAD, even, odd).astype(BF16)
    out_ref[...] = jnp.broadcast_to(attended[None], out_ref.shape)


def mix_kernel(parts_ref, w_ref, residual_ref, send_ref, mixed_ref, packed_ref, wide_ref):
    rows, chunks, lanes = parts_ref.shape
    wide_ref[...] = parts_ref[...].reshape(rows * chunks, lanes).astype(F32)
    attended = jnp.concatenate(
        [wide_ref[pl.ds(i, rows, stride=chunks), :].astype(BF16) for i in range(chunks)], axis=1
    )
    projected = jnp.dot(attended, w_ref[...], preferred_element_type=F32)
    mixed = (residual_ref[...].astype(F32) + projected).astype(BF16)
    mixed_ref[...] = mixed
    packed_ref[...] = jnp.dot(send_ref[...], mixed, preferred_element_type=F32).astype(BF16)


def hidden_kernel(parts_ref, gain_ref, w_gate_ref, w_up_ref, out_ref, inputs_ref):
    cores, chips, rows, lanes = parts_ref.shape
    squares = jnp.zeros((rows, lanes), F32)
    for core in range(cores):
        for chip in range(chips):
            part = parts_ref[core, chip].astype(F32)
            squares = squares + part * part
    mean = jnp.sum(squares, axis=-1, keepdims=True) / (cores * chips * lanes)
    scale = lax.rsqrt(mean + NORM_EPSILON)
    for core in range(cores):
        for chip in range(chips):
            first = (chip * cores + core) * lanes
            part = parts_ref[core, chip].astype(F32)
            gain = gain_ref[chip * cores + core : chip * cores + core + 1].astype(F32)
            inputs_ref[:, first : first + lanes] = (part * scale * gain).astype(BF16)
    inputs = inputs_ref[...]
    gate = jnp.dot(inputs, w_gate_ref[0], preferred_element_type=F32)
    up = jnp.dot(inputs, w_up_ref[0], preferred_element_type=F32)
    hidden = (gate / (1.0 + jnp.exp(-gate)) * up).astype(BF16)
    out_ref[...] = jnp.broadcast_to(hidden[None], out_ref.shape)


def down_kernel(parts_ref, w_ref, out_ref, hidden_ref):
    cores, peers, rows, lanes = parts_ref.shape
    for core in range(cores):
        for peer in range(peers):
            hidden_ref[core * rows : (core + 1) * rows, peer * lanes : (peer + 1) * lanes] = parts_ref[
                core, peer
            ]
    out_ref[...] = jnp.dot(hidden_ref[...], w_ref[0], preferred_element_type=F32).astype(BF16)


def combine_kernel(returned_ref, combine_ref, mixed_ref, out_ref):
    returned = returned_ref[...]
    rest = combine_ref[...]
    total = jnp.zeros(out_ref.shape, F32)
    for _ in range(3):
        part = rest.astype(BF16)
        rest = rest - part.astype(F32)
        total = total + lax.dot_general(
            part, returned, (((0,), (0,)), ((), ())), preferred_element_type=F32
        )
    out_ref[...] = (mixed_ref[...].astype(F32) + total).astype(BF16)


def solution(mesh):
    experts = mesh.shape["ep"]
    peers = mesh.shape["tp"]
    chips = peers // CORES
    split = Mesh(mesh.devices.reshape(experts, chips, CORES), ("ep", "y", "core"))
    tp = ("y", "core")

    def to_all(copies):
        exchanged = lax.all_to_all(copies, "y", 0, 0, tiled=True)
        return lax.all_gather(exchanged, "core", axis=0, tiled=False)

    def halves_to_all(copies):
        rows, lanes = copies.shape[1:]
        halves = copies.reshape(peers, rows // CORES, lanes)
        exchanged = lax.all_to_all(halves, tp, 0, 0, tiled=True)
        return lax.all_gather(exchanged, "core", axis=0, tiled=False)

    def on_device(
        tokens,
        attn_gain,
        ffn_gain,
        w_query,
        w_key,
        w_value,
        w_forget,
        forget_bias,
        w_out,
        cache_keys,
        cache_values,
        cache_logcum,
        cache_len,
        route_group,
        route_expert,
        route_weight,
        w_gate,
        w_up,
        w_down,
    ):
        rows, features = tokens.shape
        part = w_query.shape[1]
        slots = experts * TOP
        def head(*refs):
            head_kernel(*refs, per_group=experts // GROUPS)

        operands = (
            cache_len.reshape(1, 1),
            tokens,
            attn_gain.reshape(peers, part),
            w_query,
            forget_bias.reshape(1, QUERY_HEAD_COUNT),
            route_group.reshape(1, rows),
            route_expert.T,
            route_weight.T,
        )
        query, normed, bias, send, combine, used, residual = call(
            head,
            (
                held((rows, part), BF16),
                held((rows, features), BF16),
                held((QUERY_HEAD_COUNT, 128), F32),
                held((slots, rows), BF16),
                held((slots, rows), F32),
                held((8, 128), jnp.int32),
                held((rows, part), BF16),
            ),
            operands,
            [HB] * len(operands),
            scratch=[pltpu.VMEM(one.shape, one.dtype) for one in operands]
            + [pltpu.SemaphoreType.DMA((len(operands),))],
            flops=10_000_000,
            limit=HEAD_LIMIT,
        )
        query = call(
            pass_kernel,
            held((rows, part), BF16),
            (query,),
            [VM],
            flops=20_000_000_000,
        )
        own_query = lax.all_to_all(
            query.reshape(peers, 1, part), tp, split_axis=0, concat_axis=0, tiled=True
        ).reshape(peers, part)
        copies = call(
            attend_kernel,
            shaped((peers, peers, part), BF16),
            (
                used,
                own_query,
                normed,
                w_key,
                w_value,
                w_forget.T,
                bias,
                cache_keys,
                cache_values,
                cache_logcum,
            ),
            [VM] * 10,
            scratch=[pltpu.VMEM((QUERY_HEAD_COUNT, 2 * HEAD), F32)],
            flops=200_000_000,
        )
        attended = lax.all_to_all(copies, tp, 0, 0, tiled=True)
        mixed, packed = call(
            mix_kernel,
            (shaped((rows, part), BF16), shaped((slots, part), BF16)),
            (attended, w_out, residual, send),
            [VM] * 4,
            scratch=[pltpu.VMEM((rows * peers, part), F32)],
            flops=20_000_000,
        )
        arrived = lax.all_to_all(packed.reshape(experts, TOP, part), "ep", 0, 0, tiled=True)
        arrived = arrived.reshape(slots, part)
        parts = to_all(jnp.broadcast_to(arrived[None], (chips, slots, part)))
        hidden = call(
            hidden_kernel,
            shaped((chips, slots, part), BF16),
            (parts, ffn_gain.reshape(peers, part), w_gate, w_up),
            [VM] * 4,
            scratch=[pltpu.VMEM((slots, features), BF16)],
            flops=100_000_000,
        )
        result = call(
            down_kernel,
            shaped((slots, part), BF16),
            (halves_to_all(hidden), w_down),
            [VM] * 2,
            scratch=[pltpu.VMEM((slots, features), BF16)],
            flops=50_000_000,
        )
        returned = lax.all_to_all(result.reshape(experts, TOP, part), "ep", 0, 0, tiled=True)
        return call(
            combine_kernel,
            shaped((rows, part), BF16),
            (returned.reshape(slots, part), combine, mixed),
            [VM] * 3,
            flops=2_000_000,
        )

    placed = (
        P("ep", None),
        P(),
        P(),
        P(None, tp),
        P(),
        P(),
        P(),
        P(),
        P(None, tp),
        P(("ep", *tp), None, None),
        P(("ep", *tp), None, None),
        P(("ep", *tp), None, None),
        P(("ep", *tp)),
        P("ep"),
        P("ep", None),
        P("ep", None),
        P("ep", None, tp),
        P("ep", None, tp),
        P("ep", None, tp),
    )
    return jax.shard_map(
        on_device, mesh=split, in_specs=placed, out_specs=P("ep", tp), check_vma=False
    )
```

```python
import jax
import jax.numpy as jnp
from jax import lax
from jax.experimental import pallas as pl
from jax.experimental.pallas import tpu as pltpu
from jax.sharding import Mesh
from jax.sharding import PartitionSpec as P

QUERY_HEAD_COUNT = 32
KV_HEADS = 4
HEAD = 64
GROUPS = 4
TOP = 2
NORM_EPSILON = 1e-06
MASKED_SCORE = -1e30
CORES = 2
VMEM_LIMIT = 8 * 1024 * 1024
HEAD_LIMIT = 67_043_328 - 512 * 1024

F32 = jnp.float32
BF16 = jnp.bfloat16
VM = pl.BlockSpec(memory_space=pltpu.VMEM)
HB = pl.BlockSpec(memory_space=pltpu.HBM)


def call(body, outs, operands, specs, scratch=(), flops=1_000_000, moved=1_000_000, limit=VMEM_LIMIT):
    return pl.pallas_call(
        body,
        out_shape=outs,
        in_specs=specs,
        out_specs=jax.tree.map(lambda _: VM, outs),
        scratch_shapes=list(scratch),
        compiler_params=pltpu.CompilerParams(vmem_limit_bytes=limit),
        cost_estimate=pl.CostEstimate(flops=flops, bytes_accessed=moved, transcendentals=0),
    )(*operands)


def shaped(shape, dtype):
    return jax.ShapeDtypeStruct(shape, dtype)


def own_place():
    return lax.axis_index("y") * CORES + lax.axis_index("core")


def held(shape, dtype):
    return pltpu.VMEM(shape, dtype)


def head_kernel(
    length_hbm,
    tokens_hbm,
    gain_hbm,
    w_query_hbm,
    bias_hbm,
    group_hbm,
    expert_hbm,
    weight_hbm,
    query_ref,
    normed_ref,
    bias_out_ref,
    send_ref,
    combine_ref,
    used_ref,
    residual_ref,
    length_ref,
    tokens_ref,
    gain_ref,
    w_query_ref,
    bias_ref,
    group_ref,
    expert_ref,
    weight_ref,
    sems,
    *,
    per_group,
):
    sources = (
        tokens_hbm, gain_hbm, w_query_hbm, group_hbm, expert_hbm, weight_hbm, bias_hbm, length_hbm
    )
    targets = (
        tokens_ref, gain_ref, w_query_ref, group_ref, expert_ref, weight_ref, bias_ref, length_ref
    )
    loads = [
        pltpu.make_async_copy(source, target, sems.at[i])
        for i, (source, target) in enumerate(zip(sources, targets))
    ]
    for load in loads:
        load.start()
    for load in loads[:2]:
        load.wait()
    values = tokens_ref[...].astype(F32)
    rows = values.shape[0]
    mean = jnp.mean(values * values, axis=-1, keepdims=True)
    scaled = values * lax.rsqrt(mean + NORM_EPSILON)
    lanes = gain_ref.shape[1]
    normed = jnp.concatenate(
        [
            (scaled[:, i * lanes : (i + 1) * lanes] * gain_ref[i : i + 1].astype(F32)).astype(BF16)
            for i in range(gain_ref.shape[0])
        ],
        axis=1,
    )
    normed_ref[...] = normed
    place = own_place()
    first = pl.multiple_of(place * lanes, lanes)
    residual_ref[...] = tokens_ref[:, pl.ds(first, lanes)]
    for load in loads[2:]:
        load.wait()
    query_ref[...] = jnp.dot(normed, w_query_ref[...], preferred_element_type=F32).astype(BF16)

    picked = group_ref[...] * per_group + expert_ref[...]
    row_index = lax.broadcasted_iota(jnp.int32, (rows, rows), 0)
    column_index = lax.broadcasted_iota(jnp.int32, (rows, rows), 1)
    lines = [picked[j : j + 1] for j in range(TOP)]
    half = send_ref.shape[0] // TOP // 2
    in_order = [jnp.where(line < half, line + half, line - half) for line in lines]
    columns = [
        jnp.sum(jnp.where(row_index == column_index, line, 0), axis=1, keepdims=True)
        for line in lines
    ]
    slots, _ = send_ref.shape
    slot_index = lax.broadcasted_iota(jnp.int32, (slots, rows), 0)
    send = jnp.zeros((slots, rows), F32)
    combine = jnp.zeros((slots, rows), F32)
    for j in range(TOP):
        earlier = jnp.zeros((1, rows), jnp.int32)
        for other in columns:
            same = (other == lines[j]) & (row_index < column_index)
            earlier = earlier + jnp.sum(same.astype(jnp.int32), axis=0, keepdims=True)
        hit = slot_index == in_order[j] * TOP + earlier
        send = send + jnp.where(hit, 1.0, 0.0)
        combine = combine + jnp.where(hit, weight_ref[j : j + 1], 0.0)
    send_ref[...] = send.astype(BF16)
    combine_ref[...] = combine

    heads = QUERY_HEAD_COUNT
    diagonal = lax.broadcasted_iota(jnp.int32, (heads, heads), 0) == lax.broadcasted_iota(
        jnp.int32, (heads, heads), 1
    )
    bias = jnp.sum(jnp.where(diagonal, bias_ref[...], 0.0), axis=1, keepdims=True)
    bias_out_ref[...] = jnp.broadcast_to(bias, bias_out_ref.shape)
    used_ref[...] = jnp.broadcast_to(length_ref[...], used_ref.shape)


def pass_kernel(query_ref, out_ref):
    out_ref[...] = query_ref[...]


def attend_kernel(
    used_ref,
    query_ref,
    normed_ref,
    w_key_ref,
    w_value_ref,
    w_forget_ref,
    bias_ref,
    keys_ref,
    values_ref,
    cum_ref,
    out_ref,
    rows_ref,
):
    place = own_place()
    normed = normed_ref[...]
    rows = normed.shape[0]
    own_row = lax.broadcasted_iota(jnp.int32, (rows, 1), 0) == place
    own_column = lax.broadcasted_iota(jnp.int32, (1, rows), 1) == place

    def projected(w_ref):
        full = jnp.dot(normed, w_ref[...], preferred_element_type=F32)
        one = jnp.sum(jnp.where(own_row, full, 0.0), axis=0, keepdims=True)
        return one.astype(BF16).astype(F32)

    key_new = projected(w_key_ref)
    value_new = projected(w_value_ref)
    logits = lax.dot_general(
        w_forget_ref[...], normed, (((1,), (1,)), ((), ())), preferred_element_type=F32
    )
    logit = jnp.sum(jnp.where(own_column, logits, 0.0), axis=1, keepdims=True) + bias_ref[:, :1]
    log_gate = jnp.minimum(logit, 0.0) - jnp.log1p(jnp.exp(-jnp.abs(logit)))
    heads = QUERY_HEAD_COUNT
    pairs = heads // 2
    width = KV_HEADS * HEAD
    used = used_ref[:1, :1]

    def index(shape, dim):
        return lax.broadcasted_iota(jnp.int32, shape, dim)

    query = query_ref[...].astype(F32)
    rows_ref[pl.ds(0, pairs, stride=2), :] = query
    rows_ref[pl.ds(1, pairs, stride=2), :] = query
    doubled = rows_ref[...]
    odd_row = index((heads, HEAD), 0) % 2 == 1
    one_head = jnp.where(odd_row, doubled[:, HEAD:], doubled[:, :HEAD])
    in_block = index((heads, width), 1) // HEAD == index((heads, width), 0) // (heads // KV_HEADS)
    query_wide = jnp.where(in_block, jnp.concatenate([one_head] * KV_HEADS, axis=1), 0.0)
    query_all = query_wide.astype(BF16)
    scores = lax.dot_general(
        query_all, keys_ref[0], (((1,), (1,)), ((), ())), preferred_element_type=F32
    )
    cum = cum_ref[0]
    position = lax.broadcasted_iota(jnp.int32, scores.shape, 1)
    latest = jnp.sum(jnp.where(position == used - 1, cum, 0.0), axis=1, keepdims=True)
    scores = scores * (HEAD**-0.5) + latest + log_gate - cum
    usable = position < used
    scores = jnp.where(usable, scores, MASKED_SCORE)
    own = jnp.sum(query_wide * key_new, axis=1, keepdims=True) * (HEAD**-0.5)
    peak = jnp.maximum(jnp.max(scores, axis=1, keepdims=True), own)
    weights = jnp.where(usable, jnp.exp(scores - peak), 0.0)
    own_weight = jnp.exp(own - peak)
    denominator = jnp.sum(weights, axis=1, keepdims=True) + own_weight
    summed = jnp.dot(weights.astype(BF16), values_ref[0], preferred_element_type=F32)
    summed = summed + own_weight.astype(BF16).astype(F32) * value_new
    summed = jnp.where(in_block, summed, 0.0)
    summed = summed[:, : 2 * HEAD] + summed[:, 2 * HEAD :]
    summed = (summed[:, :HEAD] + summed[:, HEAD:]) / denominator
    rows_ref[...] = jnp.concatenate([summed, summed], axis=1)
    even = rows_ref[pl.ds(0, pairs, stride=2), :]
    odd = rows_ref[pl.ds(1, pairs, stride=2), :]
    attended = jnp.where(index((pairs, 2 * HEAD), 1) < HEAD, even, odd).astype(BF16)
    out_ref[...] = jnp.broadcast_to(attended[None], out_ref.shape)


def mix_kernel(parts_ref, w_ref, residual_ref, send_ref, mixed_ref, packed_ref, wide_ref):
    rows, chunks, lanes = parts_ref.shape
    wide_ref[...] = parts_ref[...].reshape(rows * chunks, lanes).astype(F32)
    attended = jnp.concatenate(
        [wide_ref[pl.ds(i, rows, stride=chunks), :].astype(BF16) for i in range(chunks)], axis=1
    )
    projected = jnp.dot(attended, w_ref[...], preferred_element_type=F32)
    mixed = (residual_ref[...].astype(F32) + projected).astype(BF16)
    mixed_ref[...] = mixed
    packed_ref[...] = jnp.dot(send_ref[...], mixed, preferred_element_type=F32).astype(BF16)


def hidden_kernel(parts_ref, gain_ref, w_gate_ref, w_up_ref, out_ref, inputs_ref):
    cores, chips, rows, lanes = parts_ref.shape
    squares = jnp.zeros((rows, lanes), F32)
    for core in range(cores):
        for chip in range(chips):
            part = parts_ref[core, chip].astype(F32)
            squares = squares + part * part
    mean = jnp.sum(squares, axis=-1, keepdims=True) / (cores * chips * lanes)
    scale = lax.rsqrt(mean + NORM_EPSILON)
    for core in range(cores):
        for chip in range(chips):
            first = (chip * cores + core) * lanes
            part = parts_ref[core, chip].astype(F32)
            gain = gain_ref[chip * cores + core : chip * cores + core + 1].astype(F32)
            inputs_ref[:, first : first + lanes] = (part * scale * gain).astype(BF16)
    inputs = inputs_ref[...]
    gate = jnp.dot(inputs, w_gate_ref[0], preferred_element_type=F32)
    up = jnp.dot(inputs, w_up_ref[0], preferred_element_type=F32)
    hidden = (gate / (1.0 + jnp.exp(-gate)) * up).astype(BF16)
    out_ref[...] = jnp.broadcast_to(hidden[None], out_ref.shape)


def down_kernel(parts_ref, w_ref, out_ref, hidden_ref):
    cores, chips, _, lanes = parts_ref.shape
    for core in range(cores):
        for i in range(chips):
            first = ((chips - 1 - i) * cores + core) * lanes
            hidden_ref[:, first : first + lanes] = parts_ref[core, i]
    out_ref[...] = jnp.dot(hidden_ref[...], w_ref[0], preferred_element_type=F32).astype(BF16)


def combine_kernel(returned_ref, combine_ref, mixed_ref, out_ref):
    returned = returned_ref[...]
    rest = combine_ref[...]
    total = jnp.zeros(out_ref.shape, F32)
    for _ in range(3):
        part = rest.astype(BF16)
        rest = rest - part.astype(F32)
        total = total + lax.dot_general(
            part, returned, (((0,), (0,)), ((), ())), preferred_element_type=F32
        )
    out_ref[...] = (mixed_ref[...].astype(F32) + total).astype(BF16)


def solution(mesh):
    experts = mesh.shape["ep"]
    peers = mesh.shape["tp"]
    chips = peers // CORES
    split = Mesh(mesh.devices.reshape(experts, chips, CORES), ("ep", "y", "core"))
    tp = ("y", "core")

    def to_all(copies, order=None):
        groups = None if order is None else [order]
        exchanged = lax.all_to_all(copies, "y", 0, 0, tiled=True, axis_index_groups=groups)
        return lax.all_gather(exchanged, "core", axis=0, tiled=False)

    chip_order = list(range(chips))[::-1]
    expert_order = [(i + experts // 2) % experts for i in range(experts)]

    def over_experts(rows):
        return lax.all_to_all(rows, "ep", 0, 0, tiled=True, axis_index_groups=[expert_order])

    def on_device(
        tokens,
        attn_gain,
        ffn_gain,
        w_query,
        w_key,
        w_value,
        w_forget,
        forget_bias,
        w_out,
        cache_keys,
        cache_values,
        cache_logcum,
        cache_len,
        route_group,
        route_expert,
        route_weight,
        w_gate,
        w_up,
        w_down,
    ):
        rows, features = tokens.shape
        part = w_query.shape[1]
        slots = experts * TOP
        def head(*refs):
            head_kernel(*refs, per_group=experts // GROUPS)

        operands = (
            cache_len.reshape(1, 1),
            tokens,
            attn_gain.reshape(peers, part),
            w_query,
            forget_bias.reshape(1, QUERY_HEAD_COUNT),
            route_group.reshape(1, rows),
            route_expert.T,
            route_weight.T,
        )
        query, normed, bias, send, combine, used, residual = call(
            head,
            (
                held((rows, part), BF16),
                held((rows, features), BF16),
                held((QUERY_HEAD_COUNT, 128), F32),
                held((slots, rows), BF16),
                held((slots, rows), F32),
                held((8, 128), jnp.int32),
                held((rows, part), BF16),
            ),
            operands,
            [HB] * len(operands),
            scratch=[pltpu.VMEM(one.shape, one.dtype) for one in operands]
            + [pltpu.SemaphoreType.DMA((len(operands),))],
            flops=10_000_000,
            limit=HEAD_LIMIT,
        )
        query = call(
            pass_kernel,
            held((rows, part), BF16),
            (query,),
            [VM],
            flops=20_000_000_000,
        )
        own_query = lax.all_to_all(
            query.reshape(peers, 1, part), tp, split_axis=0, concat_axis=0, tiled=True
        ).reshape(peers, part)
        copies = call(
            attend_kernel,
            shaped((peers, peers, part), BF16),
            (
                used,
                own_query,
                normed,
                w_key,
                w_value,
                w_forget.T,
                bias,
                cache_keys,
                cache_values,
                cache_logcum,
            ),
            [VM] * 10,
            scratch=[pltpu.VMEM((QUERY_HEAD_COUNT, 2 * HEAD), F32)],
            flops=200_000_000,
        )
        attended = lax.all_to_all(copies, tp, 0, 0, tiled=True)
        mixed, packed = call(
            mix_kernel,
            (shaped((rows, part), BF16), shaped((slots, part), BF16)),
            (attended, w_out, residual, send),
            [VM] * 4,
            scratch=[pltpu.VMEM((rows * peers, part), F32)],
            flops=20_000_000,
        )
        arrived = over_experts(packed.reshape(experts, TOP, part))
        arrived = arrived.reshape(slots, part)
        parts = to_all(jnp.broadcast_to(arrived[None], (chips, slots, part)))
        hidden = call(
            hidden_kernel,
            shaped((chips, slots, part), BF16),
            (parts, ffn_gain.reshape(peers, part), w_gate, w_up),
            [VM] * 4,
            scratch=[pltpu.VMEM((slots, features), BF16)],
            flops=100_000_000,
        )
        result = call(
            down_kernel,
            shaped((slots, part), BF16),
            (to_all(hidden, chip_order), w_down),
            [VM] * 2,
            scratch=[pltpu.VMEM((slots, features), BF16)],
            flops=50_000_000,
        )
        returned = over_experts(result.reshape(experts, TOP, part))
        return call(
            combine_kernel,
            shaped((rows, part), BF16),
            (returned.reshape(slots, part), combine, mixed),
            [VM] * 3,
            flops=2_000_000,
        )

    placed = (
        P("ep", None),
        P(),
        P(),
        P(None, tp),
        P(),
        P(),
        P(),
        P(),
        P(None, tp),
        P(("ep", *tp), None, None),
        P(("ep", *tp), None, None),
        P(("ep", *tp), None, None),
        P(("ep", *tp)),
        P("ep"),
        P("ep", None),
        P("ep", None),
        P("ep", None, tp),
        P("ep", None, tp),
        P("ep", None, tp),
    )
    return jax.shard_map(
        on_device, mesh=split, in_specs=placed, out_specs=P("ep", tp), check_vma=False
    )
```

```python
import jax
import jax.numpy as jnp
from jax import lax
from jax.experimental import pallas as pl
from jax.experimental.pallas import tpu as pltpu
from jax.sharding import Mesh
from jax.sharding import PartitionSpec as P

QUERY_HEAD_COUNT = 32
KV_HEADS = 4
HEAD = 64
GROUPS = 4
TOP = 2
NORM_EPSILON = 1e-06
MASKED_SCORE = -1e30
CORES = 2
VMEM_LIMIT = 8 * 1024 * 1024
HEAD_LIMIT = 67_043_328 - 512 * 1024

F32 = jnp.float32
BF16 = jnp.bfloat16
VM = pl.BlockSpec(memory_space=pltpu.VMEM)
HB = pl.BlockSpec(memory_space=pltpu.HBM)


def call(body, outs, operands, specs, scratch=(), flops=1_000_000, moved=1_000_000, limit=VMEM_LIMIT):
    return pl.pallas_call(
        body,
        out_shape=outs,
        in_specs=specs,
        out_specs=jax.tree.map(lambda _: VM, outs),
        scratch_shapes=list(scratch),
        compiler_params=pltpu.CompilerParams(vmem_limit_bytes=limit),
        cost_estimate=pl.CostEstimate(flops=flops, bytes_accessed=moved, transcendentals=0),
    )(*operands)


def shaped(shape, dtype):
    return jax.ShapeDtypeStruct(shape, dtype)


def own_place():
    return lax.axis_index("y") * CORES + lax.axis_index("core")


def held(shape, dtype):
    return pltpu.VMEM(shape, dtype)


def head_kernel(
    length_hbm,
    tokens_hbm,
    gain_hbm,
    w_query_hbm,
    bias_hbm,
    group_hbm,
    expert_hbm,
    weight_hbm,
    query_ref,
    normed_ref,
    bias_out_ref,
    send_ref,
    combine_ref,
    used_ref,
    residual_ref,
    length_ref,
    tokens_ref,
    gain_ref,
    w_query_ref,
    bias_ref,
    group_ref,
    expert_ref,
    weight_ref,
    sems,
    *,
    per_group,
    first_expert,
):
    sources = (
        tokens_hbm, gain_hbm, w_query_hbm, group_hbm, expert_hbm, weight_hbm, bias_hbm, length_hbm
    )
    targets = (
        tokens_ref, gain_ref, w_query_ref, group_ref, expert_ref, weight_ref, bias_ref, length_ref
    )
    loads = [
        pltpu.make_async_copy(source, target, sems.at[i])
        for i, (source, target) in enumerate(zip(sources, targets))
    ]
    for load in loads:
        load.start()
    for load in loads[:2]:
        load.wait()
    values = tokens_ref[...].astype(F32)
    rows = values.shape[0]
    mean = jnp.mean(values * values, axis=-1, keepdims=True)
    scaled = values * lax.rsqrt(mean + NORM_EPSILON)
    lanes = gain_ref.shape[1]
    normed = jnp.concatenate(
        [
            (scaled[:, i * lanes : (i + 1) * lanes] * gain_ref[i : i + 1].astype(F32)).astype(BF16)
            for i in range(gain_ref.shape[0])
        ],
        axis=1,
    )
    normed_ref[...] = normed
    place = own_place()
    first = pl.multiple_of(place * lanes, lanes)
    residual_ref[...] = tokens_ref[:, pl.ds(first, lanes)]
    for load in loads[2:]:
        load.wait()
    query_ref[...] = jnp.dot(normed, w_query_ref[...], preferred_element_type=F32).astype(BF16)

    picked = group_ref[...] * per_group + expert_ref[...]
    row_index = lax.broadcasted_iota(jnp.int32, (rows, rows), 0)
    column_index = lax.broadcasted_iota(jnp.int32, (rows, rows), 1)
    lines = [picked[j : j + 1] for j in range(TOP)]
    count = send_ref.shape[0] // TOP
    in_order = [
        jnp.where(line < first_expert, line + (count - first_expert), line - first_expert)
        for line in lines
    ]
    columns = [
        jnp.sum(jnp.where(row_index == column_index, line, 0), axis=1, keepdims=True)
        for line in lines
    ]
    slots, _ = send_ref.shape
    slot_index = lax.broadcasted_iota(jnp.int32, (slots, rows), 0)
    send = jnp.zeros((slots, rows), F32)
    combine = jnp.zeros((slots, rows), F32)
    for j in range(TOP):
        earlier = jnp.zeros((1, rows), jnp.int32)
        for other in columns:
            same = (other == lines[j]) & (row_index < column_index)
            earlier = earlier + jnp.sum(same.astype(jnp.int32), axis=0, keepdims=True)
        hit = slot_index == in_order[j] * TOP + earlier
        send = send + jnp.where(hit, 1.0, 0.0)
        combine = combine + jnp.where(hit, weight_ref[j : j + 1], 0.0)
    send_ref[...] = send.astype(BF16)
    combine_ref[...] = combine

    heads = QUERY_HEAD_COUNT
    diagonal = lax.broadcasted_iota(jnp.int32, (heads, heads), 0) == lax.broadcasted_iota(
        jnp.int32, (heads, heads), 1
    )
    bias = jnp.sum(jnp.where(diagonal, bias_ref[...], 0.0), axis=1, keepdims=True)
    bias_out_ref[...] = jnp.broadcast_to(bias, bias_out_ref.shape)
    used_ref[...] = jnp.broadcast_to(length_ref[...], used_ref.shape)


def pass_kernel(query_ref, out_ref):
    out_ref[...] = query_ref[...]


def attend_kernel(
    used_ref,
    query_ref,
    normed_ref,
    w_key_ref,
    w_value_ref,
    w_forget_ref,
    bias_ref,
    keys_ref,
    values_ref,
    cum_ref,
    out_ref,
    rows_ref,
):
    place = own_place()
    normed = normed_ref[...]
    rows = normed.shape[0]
    own_row = lax.broadcasted_iota(jnp.int32, (rows, 1), 0) == place
    own_column = lax.broadcasted_iota(jnp.int32, (1, rows), 1) == place

    def projected(w_ref):
        full = jnp.dot(normed, w_ref[...], preferred_element_type=F32)
        one = jnp.sum(jnp.where(own_row, full, 0.0), axis=0, keepdims=True)
        return one.astype(BF16).astype(F32)

    key_new = projected(w_key_ref)
    value_new = projected(w_value_ref)
    logits = lax.dot_general(
        w_forget_ref[...], normed, (((1,), (1,)), ((), ())), preferred_element_type=F32
    )
    logit = jnp.sum(jnp.where(own_column, logits, 0.0), axis=1, keepdims=True) + bias_ref[:, :1]
    log_gate = jnp.minimum(logit, 0.0) - jnp.log1p(jnp.exp(-jnp.abs(logit)))
    heads = QUERY_HEAD_COUNT
    pairs = heads // 2
    width = KV_HEADS * HEAD
    used = used_ref[:1, :1]

    def index(shape, dim):
        return lax.broadcasted_iota(jnp.int32, shape, dim)

    query = query_ref[...].astype(F32)
    rows_ref[pl.ds(0, pairs, stride=2), :] = query
    rows_ref[pl.ds(1, pairs, stride=2), :] = query
    doubled = rows_ref[...]
    odd_row = index((heads, HEAD), 0) % 2 == 1
    one_head = jnp.where(odd_row, doubled[:, HEAD:], doubled[:, :HEAD])
    in_block = index((heads, width), 1) // HEAD == index((heads, width), 0) // (heads // KV_HEADS)
    query_wide = jnp.where(in_block, jnp.concatenate([one_head] * KV_HEADS, axis=1), 0.0)
    query_all = query_wide.astype(BF16)
    scores = lax.dot_general(
        query_all, keys_ref[0], (((1,), (1,)), ((), ())), preferred_element_type=F32
    )
    cum = cum_ref[0]
    position = lax.broadcasted_iota(jnp.int32, scores.shape, 1)
    latest = jnp.sum(jnp.where(position == used - 1, cum, 0.0), axis=1, keepdims=True)
    scores = scores * (HEAD**-0.5) + latest + log_gate - cum
    usable = position < used
    scores = jnp.where(usable, scores, MASKED_SCORE)
    own = jnp.sum(query_wide * key_new, axis=1, keepdims=True) * (HEAD**-0.5)
    peak = jnp.maximum(jnp.max(scores, axis=1, keepdims=True), own)
    weights = jnp.where(usable, jnp.exp(scores - peak), 0.0)
    own_weight = jnp.exp(own - peak)
    denominator = jnp.sum(weights, axis=1, keepdims=True) + own_weight
    summed = jnp.dot(weights.astype(BF16), values_ref[0], preferred_element_type=F32)
    summed = summed + own_weight.astype(BF16).astype(F32) * value_new
    summed = jnp.where(in_block, summed, 0.0)
    summed = summed[:, : 2 * HEAD] + summed[:, 2 * HEAD :]
    summed = (summed[:, :HEAD] + summed[:, HEAD:]) / denominator
    rows_ref[...] = jnp.concatenate([summed, summed], axis=1)
    even = rows_ref[pl.ds(0, pairs, stride=2), :]
    odd = rows_ref[pl.ds(1, pairs, stride=2), :]
    attended = jnp.where(index((pairs, 2 * HEAD), 1) < HEAD, even, odd).astype(BF16)
    out_ref[...] = jnp.broadcast_to(attended[None], out_ref.shape)


def mix_kernel(parts_ref, w_ref, residual_ref, send_ref, mixed_ref, packed_ref, wide_ref):
    rows, chunks, lanes = parts_ref.shape
    wide_ref[...] = parts_ref[...].reshape(rows * chunks, lanes).astype(F32)
    attended = jnp.concatenate(
        [wide_ref[pl.ds(i, rows, stride=chunks), :].astype(BF16) for i in range(chunks)], axis=1
    )
    projected = jnp.dot(attended, w_ref[...], preferred_element_type=F32)
    mixed = (residual_ref[...].astype(F32) + projected).astype(BF16)
    mixed_ref[...] = mixed
    packed_ref[...] = jnp.dot(send_ref[...], mixed, preferred_element_type=F32).astype(BF16)


def hidden_kernel(parts_ref, gain_ref, w_gate_ref, w_up_ref, out_ref, inputs_ref):
    cores, chips, rows, lanes = parts_ref.shape
    squares = jnp.zeros((rows, lanes), F32)
    for core in range(cores):
        for chip in range(chips):
            part = parts_ref[core, chip].astype(F32)
            squares = squares + part * part
    mean = jnp.sum(squares, axis=-1, keepdims=True) / (cores * chips * lanes)
    scale = lax.rsqrt(mean + NORM_EPSILON)
    for core in range(cores):
        for chip in range(chips):
            first = (chip * cores + core) * lanes
            part = parts_ref[core, chip].astype(F32)
            gain = gain_ref[chip * cores + core : chip * cores + core + 1].astype(F32)
            inputs_ref[:, first : first + lanes] = (part * scale * gain).astype(BF16)
    inputs = inputs_ref[...]
    gate = jnp.dot(inputs, w_gate_ref[0], preferred_element_type=F32)
    up = jnp.dot(inputs, w_up_ref[0], preferred_element_type=F32)
    hidden = (gate / (1.0 + jnp.exp(-gate)) * up).astype(BF16)
    out_ref[...] = jnp.broadcast_to(hidden[None], out_ref.shape)


def down_kernel(parts_ref, w_ref, out_ref, hidden_ref, *, chip_order):
    cores, _, _, lanes = parts_ref.shape
    for core in range(cores):
        for i, chip in enumerate(chip_order):
            first = (chip * cores + core) * lanes
            hidden_ref[:, first : first + lanes] = parts_ref[core, i]
    out_ref[...] = jnp.dot(hidden_ref[...], w_ref[0], preferred_element_type=F32).astype(BF16)


def combine_kernel(returned_ref, combine_ref, mixed_ref, out_ref):
    returned = returned_ref[...]
    rest = combine_ref[...]
    total = jnp.zeros(out_ref.shape, F32)
    for _ in range(3):
        part = rest.astype(BF16)
        rest = rest - part.astype(F32)
        total = total + lax.dot_general(
            part, returned, (((0,), (0,)), ((), ())), preferred_element_type=F32
        )
    out_ref[...] = (mixed_ref[...].astype(F32) + total).astype(BF16)


def solution(mesh):
    experts = mesh.shape["ep"]
    peers = mesh.shape["tp"]
    chips = peers // CORES
    split = Mesh(mesh.devices.reshape(experts, chips, CORES), ("ep", "y", "core"))
    tp = ("y", "core")

    def to_all(copies, order=None):
        groups = None if order is None else [order]
        exchanged = lax.all_to_all(copies, "y", 0, 0, tiled=True, axis_index_groups=groups)
        return lax.all_gather(exchanged, "core", axis=0, tiled=False)

    chip_order = [*range(chips - 2, -1, -1), chips - 1]
    first_expert = experts * 7 // 12
    expert_order = [(i + first_expert) % experts for i in range(experts)]

    def over_experts(rows):
        return lax.all_to_all(rows, "ep", 0, 0, tiled=True, axis_index_groups=[expert_order])

    def on_device(
        tokens,
        attn_gain,
        ffn_gain,
        w_query,
        w_key,
        w_value,
        w_forget,
        forget_bias,
        w_out,
        cache_keys,
        cache_values,
        cache_logcum,
        cache_len,
        route_group,
        route_expert,
        route_weight,
        w_gate,
        w_up,
        w_down,
    ):
        rows, features = tokens.shape
        part = w_query.shape[1]
        slots = experts * TOP
        def head(*refs):
            head_kernel(*refs, per_group=experts // GROUPS, first_expert=first_expert)

        operands = (
            cache_len.reshape(1, 1),
            tokens,
            attn_gain.reshape(peers, part),
            w_query,
            forget_bias.reshape(1, QUERY_HEAD_COUNT),
            route_group.reshape(1, rows),
            route_expert.T,
            route_weight.T,
        )
        query, normed, bias, send, combine, used, residual = call(
            head,
            (
                held((rows, part), BF16),
                held((rows, features), BF16),
                held((QUERY_HEAD_COUNT, 128), F32),
                held((slots, rows), BF16),
                held((slots, rows), F32),
                held((8, 128), jnp.int32),
                held((rows, part), BF16),
            ),
            operands,
            [HB] * len(operands),
            scratch=[pltpu.VMEM(one.shape, one.dtype) for one in operands]
            + [pltpu.SemaphoreType.DMA((len(operands),))],
            flops=10_000_000,
            limit=HEAD_LIMIT,
        )
        query = call(
            pass_kernel,
            held((rows, part), BF16),
            (query,),
            [VM],
            flops=20_000_000_000,
        )
        own_query = lax.all_to_all(
            query.reshape(peers, 1, part), tp, split_axis=0, concat_axis=0, tiled=True
        ).reshape(peers, part)
        copies = call(
            attend_kernel,
            shaped((peers, peers, part), BF16),
            (
                used,
                own_query,
                normed,
                w_key,
                w_value,
                w_forget.T,
                bias,
                cache_keys,
                cache_values,
                cache_logcum,
            ),
            [VM] * 10,
            scratch=[pltpu.VMEM((QUERY_HEAD_COUNT, 2 * HEAD), F32)],
            flops=200_000_000,
        )
        attended = lax.all_to_all(copies, tp, 0, 0, tiled=True)
        mixed, packed = call(
            mix_kernel,
            (shaped((rows, part), BF16), shaped((slots, part), BF16)),
            (attended, w_out, residual, send),
            [VM] * 4,
            scratch=[pltpu.VMEM((rows * peers, part), F32)],
            flops=20_000_000,
        )
        arrived = over_experts(packed.reshape(experts, TOP, part))
        arrived = arrived.reshape(slots, part)
        parts = to_all(jnp.broadcast_to(arrived[None], (chips, slots, part)))
        hidden = call(
            hidden_kernel,
            shaped((chips, slots, part), BF16),
            (parts, ffn_gain.reshape(peers, part), w_gate, w_up),
            [VM] * 4,
            scratch=[pltpu.VMEM((slots, features), BF16)],
            flops=100_000_000,
        )
        def down(*refs):
            down_kernel(*refs, chip_order=chip_order)

        result = call(
            down,
            shaped((slots, part), BF16),
            (to_all(hidden, chip_order), w_down),
            [VM] * 2,
            scratch=[pltpu.VMEM((slots, features), BF16)],
            flops=50_000_000,
        )
        returned = over_experts(result.reshape(experts, TOP, part))
        return call(
            combine_kernel,
            shaped((rows, part), BF16),
            (returned.reshape(slots, part), combine, mixed),
            [VM] * 3,
            flops=2_000_000,
        )

    placed = (
        P("ep", None),
        P(),
        P(),
        P(None, tp),
        P(),
        P(),
        P(),
        P(),
        P(None, tp),
        P(("ep", *tp), None, None),
        P(("ep", *tp), None, None),
        P(("ep", *tp), None, None),
        P(("ep", *tp)),
        P("ep"),
        P("ep", None),
        P("ep", None),
        P("ep", None, tp),
        P("ep", None, tp),
        P("ep", None, tp),
    )
    return jax.shard_map(
        on_device, mesh=split, in_specs=placed, out_specs=P("ep", tp), check_vma=False
    )
```
